32 devices in a mesh: sp: 4 (over y, x), tp: 8 (over z, core).
Axes of the slice: x: 2, y: 2, z: 4, core: 2. Of those that a mesh axis runs over, the one named last changes fastest.
Arguments:
- residual_in: bfloat16 [1024, 4096], P(('sp', 'tp')), may hold values from -6 to 6
- queries: bfloat16 [1024, 2048], P('sp', 'tp'), may hold values from -6 to 6
- keys: bfloat16 [1024, 2048], P('sp', 'tp'), may hold values from -6 to 6
- values: bfloat16 [1024, 2048], P('sp', 'tp'), may hold values from -6 to 6
- break_offset: bfloat16 [1024, 32], P('sp', 'tp'), may hold values from -14 to 1
- doc_ids: int32 [1024], P('sp'), may hold values from 0 to 2, never falling along the last dimension, each value on 1 to 640 neighbouring positions
- out_weight: bfloat16 [2048, 4096], P('tp'), may hold values from -0.125 to 0.125
- norm_gain: float32 [4096], replicated, may hold values from 0.1 to 1.9
- group_router: bfloat16 [4096, 2], replicated, may hold values from -0.1875 to 0.1875
- expert_router: bfloat16 [4096, 4], replicated, may hold values from -0.1875 to 0.1875
- expert_ids: int32 [1024, 2], P('sp'), may hold values from 0 to 3, as said below
- gate_weight: bfloat16 [4, 4096, 4096], P('sp', None, 'tp'), may hold values from -0.09375 to 0.09375
- up_weight: bfloat16 [4, 4096, 4096], P('sp', None, 'tp'), may hold values from -0.09375 to 0.09375
- down_weight: bfloat16 [4, 4096, 4096], P('sp', 'tp'), may hold values from -0.09375 to 0.09375
Outputs:
- layer_out: bfloat16 [1024, 4096], P(('sp', 'tp'))
The draws below stay inside these ranges and needn't reach their ends.
Inputs may be any that keep to these rules, and one draw needn't show every extreme that they name: `doc_ids`: document numbers never fall along the positions; one document covers exactly 640 positions. `expert_ids`: the two experts of a position differ and lie in one group of 2 consecutive numbers; in each aligned block of 32 positions every expert is named exactly 16 times.
All inputs are finite; a program needn't handle non-finite values.
Results may differ from the reference program's by a relative error of at most 0.013.
Values may be sent and summed in bfloat16 or wider, within the bound.
A program may use at most 64 MiB of HBM per device.

```python
import math
import jax
import jax.numpy as jnp
import numpy as np
from jax import lax

D = 4096
ATTENTION_HEADS = 32
HEAD_DIM = 64
ATT = 2048
D_EXPERT = 4096
GROUPS = 2
EXPERTS = 4
GROUP_EXPERTS = 2
TOK_DEV = 256
SEQUENCE_TOKENS = 1024
ROWS_DEV = 32
KEY_BLOCK = 256
DOCS = 3
DOC_MOST = 640
N_TP = 8


def draw_break_offset(key, part):
    gathered_keys = jax.random.split(jax.random.fold_in(key, 7), 5)
    lagging_heads = jax.random.uniform(gathered_keys[0], (ATTENTION_HEADS,)) < 0.5
    factor = jnp.exp(jax.random.uniform(gathered_keys[1], (SEQUENCE_TOKENS // TOK_DEV, 1), minval=0.0, maxval=math.log(4.0)))
    factor = jnp.repeat(factor, TOK_DEV, axis=0)
    slow_level = jnp.log(0.1 * factor / SEQUENCE_TOKENS)
    fast_level = jnp.log(factor / 48.0)
    jitter = 0.5 * jax.random.normal(gathered_keys[2], (SEQUENCE_TOKENS, ATTENTION_HEADS))
    logging_level = jnp.where(lagging_heads[None, :], slow_level, fast_level) + jitter
    spike_matched = jax.random.uniform(gathered_keys[3], (SEQUENCE_TOKENS, ATTENTION_HEADS)) < 6.0 / SEQUENCE_TOKENS
    spike_value = jax.random.uniform(gathered_keys[4], (SEQUENCE_TOKENS, ATTENTION_HEADS), minval=-1.0, maxval=0.0)
    document_starts = jnp.where(spike_matched & lagging_heads[None, :], spike_value, logging_level)
    return jnp.clip(document_starts, -14.0, 1.0).astype(jnp.bfloat16)


def draw_expert_ids(key, part):
    routing_key = jax.random.fold_in(key, 13)
    blocks = SEQUENCE_TOKENS // ROWS_DEV
    per_group = ROWS_DEV // GROUPS
    group_size = EXPERTS // GROUPS
    block_keys = jax.random.split(routing_key, blocks)

    def one_block(block_key):
        perm_key, relabel_key, swap_key = jax.random.split(block_key, 3)
        row_rank = jax.random.permutation(perm_key, ROWS_DEV)
        group_index = row_rank // per_group
        inner_rank = row_rank % per_group
        relabel = jax.vmap(lambda sub_key: jax.random.permutation(sub_key, group_size))(jax.random.split(relabel_key, GROUPS))
        first = relabel[group_index, inner_rank % group_size]
        second = relabel[group_index, (inner_rank + 1) % group_size]
        swapped = jax.random.randint(swap_key, (ROWS_DEV,), 0, 2)
        lower_id = jnp.where(swapped == 1, second, first)
        upper_id = jnp.where(swapped == 1, first, second)
        return jnp.stack([group_index * group_size + lower_id, group_index * group_size + upper_id], axis=1)
    return jax.vmap(one_block)(block_keys).reshape(SEQUENCE_TOKENS, 2).astype(jnp.int32)


def block_levels(key, shape, shards, smallest, largest):
    loudness, own = 1.0, jax.random.fold_in(key, 6)
    for axis_at, blocks in shards:
        draws = jnp.exp(jax.random.uniform(jax.random.fold_in(own, axis_at), (blocks,), jnp.float32, smallest / len(shards), largest / len(shards)))
        loudness = loudness * jnp.repeat(draws, shape[axis_at] // blocks).reshape([-1 if axis == axis_at else 1 for axis in range(len(shape))])
    return loudness


def profile(amount, total, bound, skew):
    portions = [(1 << 20) // math.isqrt(grade ** skew) + 1 for grade in range(2, amount + 1)]
    surplus, holding = total - bound - (amount - 1), [1] * (amount - 1)
    while surplus > 0:
        movable = [i for i in range(amount - 1) if holding[i] < bound]
        mass, left = sum([portions[i] for i in movable]), surplus
        for i in movable:
            extra = min(bound - holding[i], max(1, left * portions[i] // mass), surplus)
            holding[i] = holding[i] + extra
            surplus = surplus - extra
    return np.array([bound] + holding)


def ragged(rng, amount, total, bound, lean):
    if amount == 2:
        one = jax.random.randint(rng, (), max(1, total - bound), min(bound, total - 1) + 1)
        return jnp.stack([one, total - one])
    lengths = jnp.asarray(profile(amount, total, bound, lean), jnp.int32)
    twos = (amount - 1) // 2
    donor, sink = lengths[1:1 + 2 * twos:2], lengths[2:2 + 2 * twos:2]
    room = jnp.minimum(donor - 1, bound - sink)
    passed = jax.random.randint(jax.random.fold_in(rng, 1), (twos,), 0, 1 << 20) % (room + 1)
    lengths = lengths.at[1:1 + 2 * twos:2].set(donor - passed).at[2:2 + 2 * twos:2].set(sink + passed)
    return lengths[jax.random.permutation(jax.random.fold_in(rng, 2), amount)]


def gaussian(stream_key, dims, width, bound, cuts=(), held_as=jnp.bfloat16):
    result = jax.random.normal(stream_key, dims, jnp.float32) * width
    if len(cuts) > 0:
        result = block_levels(stream_key, dims, cuts, -0.22, 0.18) * result
    return jnp.clip(result, min=-bound, max=bound).astype(held_as)


def setup_inputs(seed: int = 0) -> dict:
    seeds = jax.random.split(jax.random.key(seed), 15)
    return {
        "residual_in": gaussian(seeds[0], (SEQUENCE_TOKENS, D), 1.0, 6.0, ((0, 32),)),
        "queries": gaussian(seeds[1], (SEQUENCE_TOKENS, ATT), 1.0, 6.0, ((0, 4), (1, 8))),
        "keys": gaussian(seeds[2], (SEQUENCE_TOKENS, ATT), 1.0, 6.0, ((0, 4), (1, 8))),
        "values": gaussian(seeds[3], (SEQUENCE_TOKENS, ATT), 1.0, 6.0, ((0, 4), (1, 8))),
        "break_offset": draw_break_offset(jax.random.fold_in(seeds[14], 71), 0),
        "doc_ids": jnp.searchsorted(jnp.cumsum(ragged(seeds[5], DOCS, SEQUENCE_TOKENS, DOC_MOST, 0)), jnp.arange(SEQUENCE_TOKENS), side="right").astype(jnp.int32),
        "out_weight": gaussian(seeds[6], (ATT, D), ATT ** -0.5, 0.125, ((0, 8),)),
        "norm_gain": jnp.clip(1.0 + 0.18 * jax.random.normal(seeds[7], (D,), jnp.float32), 0.1, 1.9),
        "group_router": gaussian(seeds[8], (D, GROUPS), (D // 4) ** -0.5, 0.1875),
        "expert_router": gaussian(seeds[9], (D, EXPERTS), (D // 4) ** -0.5, 0.1875),
        "expert_ids": draw_expert_ids(jax.random.fold_in(seeds[14], 71), 0),
        "gate_weight": gaussian(seeds[11], (EXPERTS, D, D_EXPERT), D ** -0.5, 0.09375, ((0, 4), (2, 8))),
        "up_weight": gaussian(seeds[12], (EXPERTS, D, D_EXPERT), D ** -0.5, 0.09375, ((0, 4), (2, 8))),
        "down_weight": gaussian(seeds[13], (EXPERTS, D_EXPERT, D), D_EXPERT ** -0.5, 0.09375, ((0, 4), (1, 8))),
    }


def block_result(query_head, key_block, value_block, offset_block, query_pos, query_doc, key_pos, key_doc):
    scores = jnp.dot(query_head, key_block.T, preferred_element_type=jnp.float32) * HEAD_DIM ** (-0.5)
    scores = scores + offset_block.astype(jnp.float32)[None, :]
    live_mask = (key_pos[None, :] < query_pos[:, None]) & (key_doc[None, :] == query_doc[:, None])
    stay_log = jnp.where(live_mask, jax.nn.log_sigmoid(-scores), jnp.float32(0.0))
    within = lax.cumsum(stay_log, axis=1, reverse=True) - stay_log
    weights = jnp.where(live_mask, jnp.exp(jax.nn.log_sigmoid(scores) + within), jnp.float32(0.0)).astype(jnp.bfloat16)
    partial_out = jnp.dot(weights, value_block, preferred_element_type=jnp.float32)
    return (partial_out, lax.optimization_barrier(jnp.sum(stay_log, axis=1)))

def attend(queries, keys, values, break_offset, doc_ids):
    positions = jnp.arange(SEQUENCE_TOKENS, dtype=jnp.int32)
    query_heads = queries.reshape(SEQUENCE_TOKENS, ATTENTION_HEADS, HEAD_DIM).transpose(1, 0, 2)
    key_heads = keys.reshape(SEQUENCE_TOKENS, ATTENTION_HEADS, HEAD_DIM).transpose(1, 0, 2)
    value_heads = values.reshape(SEQUENCE_TOKENS, ATTENTION_HEADS, HEAD_DIM).transpose(1, 0, 2)
    document_starts = break_offset.T
    block_count = SEQUENCE_TOKENS // KEY_BLOCK

    def one_head(operands):
        query_head, key_head, value_head, offset_head = operands

        def advance(running, block_index):
            out_sum, stay_sum = running
            block_begin = (block_index * KEY_BLOCK).astype(jnp.int32)
            key_block = lax.dynamic_slice_in_dim(key_head, block_begin, KEY_BLOCK, 0)
            value_block = lax.dynamic_slice_in_dim(value_head, block_begin, KEY_BLOCK, 0)
            offset_block = lax.dynamic_slice_in_dim(offset_head, block_begin, KEY_BLOCK, 0)
            key_doc = lax.dynamic_slice_in_dim(doc_ids, block_begin, KEY_BLOCK, 0)
            key_pos = block_begin + jnp.arange(KEY_BLOCK, dtype=jnp.int32)
            partial_out, totals = block_result(query_head, key_block, value_block, offset_block, positions, doc_ids, key_pos, key_doc)
            out_sum = out_sum + jnp.exp(stay_sum)[:, None] * partial_out
            return ((out_sum, stay_sum + totals), None)
        initial = (jnp.zeros((SEQUENCE_TOKENS, HEAD_DIM), jnp.float32), jnp.zeros((SEQUENCE_TOKENS,), jnp.float32))
        final, unused = lax.scan(advance, initial, jnp.arange(block_count, dtype=jnp.int32), reverse=True)
        return final[0]
    mixed = lax.map(one_head, (query_heads, key_heads, value_heads, document_starts))
    return mixed.transpose(1, 0, 2).reshape(SEQUENCE_TOKENS, ATTENTION_HEADS * HEAD_DIM).astype(jnp.bfloat16)

def reference(residual_in, queries, keys, values, break_offset, doc_ids, out_weight, norm_gain, group_router, expert_router, expert_ids, gate_weight, up_weight, down_weight):
    attended = attend(queries, keys, values, break_offset, doc_ids)
    width_part = ATTENTION_HEADS * HEAD_DIM // N_TP

    def add_group(running, group_index):
        block_begin = (group_index * width_part).astype(jnp.int32)
        part_in = lax.dynamic_slice_in_dim(attended, block_begin, width_part, 1)
        part_weight = lax.dynamic_slice_in_dim(out_weight, block_begin, width_part, 0)
        product = lax.optimization_barrier(jnp.dot(part_in, part_weight, preferred_element_type=jnp.float32).astype(jnp.bfloat16))
        return (running + product.astype(jnp.float32), None)
    summed, unused = lax.scan(add_group, residual_in.astype(jnp.float32), jnp.arange(N_TP, dtype=jnp.int32))
    mixed_stream = summed.astype(jnp.bfloat16)
    stream_f = mixed_stream.astype(jnp.float32)
    scaling = lax.rsqrt(lax.optimization_barrier(jnp.mean(stream_f * stream_f, axis=1, keepdims=True)) + 1e-06)
    normed = (stream_f * scaling * norm_gain[None, :]).astype(jnp.bfloat16)
    group_logits = jnp.dot(normed, group_router, preferred_element_type=jnp.float32)
    expert_logits = jnp.dot(normed, expert_router, preferred_element_type=jnp.float32)
    chosen_group = expert_ids[:, 0] // GROUP_EXPERTS
    margin = group_logits[:, 0] - group_logits[:, 1]
    own_margin = jnp.where(chosen_group == 0, margin, -margin)
    picked = jnp.take_along_axis(expert_logits, expert_ids, axis=1)
    routes = jax.nn.sigmoid(own_margin)[:, None] * jax.nn.sigmoid(picked - picked[:, ::-1])
    flat_ids = expert_ids.reshape(-1)
    per_expert = 2 * SEQUENCE_TOKENS // EXPERTS
    slice_units = D_EXPERT // N_TP

    def one_expert(operands):
        expert_index, gate_part, up_part, down_part = operands
        row_index = jnp.nonzero(flat_ids == expert_index, size=per_expert)[0].astype(jnp.int32)
        row_block = normed[row_index // 2]
        gate_val = jnp.dot(row_block, gate_part, preferred_element_type=jnp.float32)
        up_val = jnp.dot(row_block, up_part, preferred_element_type=jnp.float32)
        hidden = (jax.nn.silu(gate_val) * up_val).astype(jnp.bfloat16)

        def add_slice(running, slice_index):
            block_begin = (slice_index * slice_units).astype(jnp.int32)
            part_hidden = lax.dynamic_slice_in_dim(hidden, block_begin, slice_units, 1)
            part_down = lax.dynamic_slice_in_dim(down_part, block_begin, slice_units, 0)
            product = lax.optimization_barrier(jnp.dot(part_hidden, part_down, preferred_element_type=jnp.float32).astype(jnp.bfloat16))
            return (running + product.astype(jnp.float32), None)
        initial = jnp.zeros((per_expert, D), jnp.float32)
        total_out, unused_slices = lax.scan(add_slice, initial, jnp.arange(N_TP, dtype=jnp.int32))
        return (total_out.astype(jnp.bfloat16), row_index)
    outputs, indices = lax.map(one_expert, (jnp.arange(EXPERTS, dtype=jnp.int32), gate_weight, up_weight, down_weight))
    expert_out = jnp.zeros((SEQUENCE_TOKENS * 2, D), jnp.bfloat16).at[indices.reshape(-1)].set(outputs.reshape(-1, D))
    expert_out = expert_out.reshape(SEQUENCE_TOKENS, 2, D)
    mixture = lax.optimization_barrier(jnp.sum(routes[:, :, None] * expert_out.astype(jnp.float32), axis=1))
    return (stream_f + mixture).astype(jnp.bfloat16)
```

```python
import functools

import jax
import jax.numpy as jnp
from jax import lax
from jax.experimental import pallas as pl
from jax.experimental.pallas import tpu as pltpu
from jax.sharding import PartitionSpec as P

HEAD_DIM = 64
PIECES = 4
GROUPS = 2


def route_weights(normed, group_router, expert_router, chosen, group_size):
    group_logits = jnp.dot(normed, group_router, preferred_element_type=jnp.float32)
    expert_logits = jnp.dot(normed, expert_router, preferred_element_type=jnp.float32)
    chosen_group = chosen[:, 0] // group_size
    margin = group_logits[:, 0] - group_logits[:, 1]
    own_margin = jnp.where(chosen_group == 0, margin, -margin)
    experts_iota = jnp.arange(expert_logits.shape[1], dtype=jnp.int32)
    picked = jnp.sum(
        jnp.where(
            chosen[:, :, None] == experts_iota[None, None, :],
            expert_logits[:, None, :],
            jnp.float32(0.0),
        ),
        axis=2,
    )
    return jax.nn.sigmoid(own_margin)[:, None] * jax.nn.sigmoid(picked - picked[:, ::-1])


def slot_table(chosen, expert_count, slots):
    flat_ids = chosen.reshape(-1)
    onehot = (flat_ids[:, None] == jnp.arange(expert_count, dtype=jnp.int32)[None, :]).astype(
        jnp.int32
    )
    before = jnp.cumsum(onehot, axis=0) - onehot
    ranks = jnp.sum(before * onehot, axis=1)
    return (flat_ids * slots + ranks).reshape(chosen.shape)


def dispatch(normed, slot_ids, total_slots):
    flat_slots = slot_ids.reshape(-1)
    owners = jnp.arange(flat_slots.shape[0], dtype=jnp.int32) // 2
    slot_iota = jnp.arange(total_slots, dtype=jnp.int32)
    token_of_slot = jnp.sum(
        jnp.where(slot_iota[:, None] == flat_slots[None, :], owners[None, :], 0), axis=1
    )
    return jnp.take(normed, token_of_slot, axis=0)


def expert_rows(row_block, gate_part, up_part, down_part):
    gate_val = jnp.dot(row_block, gate_part, preferred_element_type=jnp.float32)
    up_val = jnp.dot(row_block, up_part, preferred_element_type=jnp.float32)
    hidden = (jax.nn.silu(gate_val) * up_val).astype(jnp.bfloat16)
    return jnp.dot(hidden, down_part, preferred_element_type=jnp.float32).astype(jnp.bfloat16)


MESH_ID = pl.DeviceIdType.MESH
VMEM_SPEC = pl.BlockSpec(memory_space=pltpu.VMEM)
ANY_SPEC = pl.BlockSpec(memory_space=pl.ANY)
F32 = jnp.float32
BF16 = jnp.bfloat16


def remote(src, dst, send_sem, recv_sem, device):
    return pltpu.make_async_remote_copy(
        src_ref=src, dst_ref=dst, send_sem=send_sem, recv_sem=recv_sem,
        device_id=device, device_id_type=MESH_ID,
    )


def columns(piece, width):
    return pl.ds((piece % 2) * (width // 2), width // 2)


def greet(device):
    pl.semaphore_signal(
        pltpu.get_barrier_semaphore(), inc=1, device_id=device, device_id_type=MESH_ID
    )


def line_reduce(
    chips, chip, sp, tp, block, down_in, up_in, sems, ready=None, finished=None, near_first=False
):
    down_send, down_recv, up_send, up_recv = sems

    def step(dest, half, arrives, inbox, send, recv, device, wait_only):
        piece = block(dest, half)
        copy = remote(piece, inbox.at[dest, half], send.at[dest, half], recv.at[dest, half], device)
        if wait_only:
            copy.wait_send()
            return
        if ready is not None:
            ready(dest, half)

        @pl.when(arrives)
        def _():
            copy.wait_recv()
            piece[...] = (piece[...].astype(F32) + inbox[dest, half].astype(F32)).astype(BF16)

        copy.start()

    def sweep(wait_only):
        for turn in range(1, 2 * chips - 2 if near_first else chips):
            if near_first:
                below, above = 2 * (chips - 1) - turn - chip, turn - chip
            else:
                below, above = chip - (chips - turn), chip + (chips - turn)
            for half in range(PIECES):

                @pl.when((below >= 0) & (below < chip))
                def _():
                    step(below, half, chip < chips - 1, down_in, down_send, down_recv,
                         (sp, tp - 2), wait_only)

                @pl.when((above > chip) & (above < chips))
                def _():
                    step(above, half, chip > 0, up_in, up_send, up_recv,
                         (sp, tp + 2), wait_only)

    sweep(False)
    for half in range(PIECES):
        if ready is not None:
            ready(chip, half)
        piece = block(chip, half)
        for arrives, inbox, recv, send in (
            (chip < chips - 1, down_in, down_recv, down_send),
            (chip > 0, up_in, up_recv, up_send),
        ):

            @pl.when(arrives)
            def _():
                remote(piece, inbox.at[chip, half], send.at[chip, half], recv.at[chip, half],
                       (sp, tp)).wait_recv()
                piece[...] = (piece[...].astype(F32) + inbox[chip, half].astype(F32)).astype(BF16)

        if finished is not None:
            finished(half)

    return lambda: sweep(True)


def mixer_kernel(
    sp_count, chips, heads, loads, later_loads,
    q_ref, k_ref, v_ref, off_ref, doc_ref, res_ref, gain_ref, w_hbm,
    mixed_ref, normed_ref,
    meta_ref, doc_col, k_buf, v_buf, m_buf, acc, carry, w_buf, part, partner_in, down_in, up_in,
    w_sem, kv_send, kv_recv, p_send, p_recv, down_send, down_recv, up_send, up_recv,
):
    sp = lax.axis_index("sp")
    tp = lax.axis_index("tp")
    chip = tp // 2
    core = tp % 2
    partner = tp + 1 - 2 * core
    tok, att = q_ref.shape
    width = res_ref.shape[1]
    half_rows = res_ref.shape[0] // 2

    w_copy = pltpu.make_async_copy(w_hbm, w_buf, w_sem)
    for j in range(1, sp_count):
        greet((lax.rem(sp + j, sp_count), tp))
    greet((sp, partner))

    @pl.when(chip > 0)
    def _():
        greet((sp, tp - 2))

    @pl.when(chip < chips - 1)
    def _():
        greet((sp, tp + 2))

    expect = sp_count + jnp.where(chip > 0, 1, 0) + jnp.where(chip < chips - 1, 1, 0)
    docs = doc_ref[...].astype(F32)
    meta_ref[...] = jnp.zeros_like(meta_ref)
    meta_ref[0:heads, :] = off_ref[...].astype(F32)
    meta_ref[heads : heads + 1, :] = docs
    doc_col[...] = jnp.broadcast_to(docs, (128, tok)).T[:, :1]
    for copy in loads:
        copy.wait()
    pl.semaphore_wait(pltpu.get_barrier_semaphore(), expect)

    def kv_copies(j, target):
        return [
            remote(src, buf.at[j - 1], kv_send.at[j - 1, n], kv_recv.at[j - 1, n], (target, tp))
            for n, (src, buf) in enumerate(((k_ref, k_buf), (v_ref, v_buf), (meta_ref, m_buf)))
        ]

    for j in range(1, sp_count):

        @pl.when(sp + j < sp_count)
        def _():
            for copy in kv_copies(j, sp + j):
                copy.start()

    w_copy.start()
    for copy in later_loads:
        copy.start()

    row = lax.broadcasted_iota(jnp.int32, (tok, tok), 0)
    col = lax.broadcasted_iota(jnp.int32, (tok, tok), 1)
    later = jnp.where(row > col, 1.0, 0.0).astype(BF16)
    lane = lax.broadcasted_iota(jnp.int32, (tok, att), 1) // HEAD_DIM
    acc[...] = jnp.zeros_like(acc)
    carry[...] = jnp.zeros_like(carry)

    def attend_block(keys, vals, meta, own):
        live = doc_col[...] == meta[heads : heads + 1, :]
        if own:
            live = live & (col < row)
        for h in range(heads):
            queries = jnp.where(lane == h, q_ref[...], jnp.zeros((), BF16)) * jnp.asarray(
                HEAD_DIM ** (-0.5), BF16
            )
            scores = lax.dot_general(
                queries, keys, (((1,), (1,)), ((), ())), preferred_element_type=F32
            ) + meta[h : h + 1, :]
            soft = jnp.maximum(scores, 0.0) + jnp.log(1.0 + jnp.exp(-jnp.abs(scores)))
            stay = jnp.where(live, -soft, 0.0)
            high = stay.astype(BF16)
            low = (stay - high.astype(F32)).astype(BF16)
            within = jnp.dot(high, later, preferred_element_type=F32) + jnp.dot(
                low, later, preferred_element_type=F32
            )
            before = carry[h]
            weights = jnp.where(
                live, jnp.exp(scores - soft + within + before), 0.0
            ).astype(BF16)
            out = jnp.dot(weights, vals, preferred_element_type=F32)
            acc[...] += jnp.where(lane == h, out, 0.0)
            carry[h] = before + within[:, :1] + stay[:, :1]

    attend_block(k_ref[...], v_ref[...], meta_ref[...], True)

    def earlier(j, unused):
        @pl.when(sp - j >= 0)
        def _():
            for copy in kv_copies(j, sp):
                copy.wait_recv()
            attend_block(k_buf[j - 1], v_buf[j - 1], m_buf[j - 1], False)

        return unused

    lax.fori_loop(1, sp_count, earlier, 0)
    for j in range(1, sp_count):

        @pl.when(sp + j < sp_count)
        def _():
            for copy in kv_copies(j, sp + j):
                copy.wait_send()

    w_copy.wait()
    attended = acc[...].astype(BF16)
    tile = 512
    for n in range(width // tile):
        cols = slice(n * tile, (n + 1) * tile)
        product = jnp.dot(attended, w_buf[:, cols], preferred_element_type=F32).astype(BF16)
        for z in range(chips):
            for c in range(2):
                for s in range(2):
                    at = ((z * 2 + c) * 2 + s) * half_rows
                    part[c, z, s, :, cols] = product[at : at + half_rows]

    def p_copy(z):
        return remote(
            part.at[1 - core, z], partner_in.at[z], p_send.at[z], p_recv.at[z], (sp, partner)
        )

    for z in range(chips):
        p_copy(z).start()
    for z in range(chips):
        p_copy(z).wait_recv()
        part[core, z] = (part[core, z].astype(F32) + partner_in[z].astype(F32)).astype(BF16)
    finish = line_reduce(
        chips, chip, sp, tp, lambda z, p: part.at[core, z, p // 2, :, columns(p, width)], down_in, up_in,
        (down_send, down_recv, up_send, up_recv),
    )
    for copy in later_loads[:1]:
        copy.wait()
    total = part[core, chip].reshape(res_ref.shape).astype(F32)
    mixed = (res_ref[...].astype(F32) + total).astype(BF16)
    mixed_ref[...] = mixed
    mixed_f = mixed.astype(F32)
    scaling = lax.rsqrt(jnp.mean(mixed_f * mixed_f, axis=1, keepdims=True) + 1e-06)
    normed_ref[...] = (mixed_f * scaling * gain_ref[...]).astype(BF16)
    for z in range(chips):
        p_copy(z).wait_send()
    finish()


def mixer_scratch(residual, queries, heads, out_weight):
    sp_count = lax.axis_size("sp")
    chips = lax.axis_size("tp") // 2
    rows, width = residual.shape
    tok, att = queries.shape
    others = max(sp_count - 1, 1)
    half = (chips, 2, rows // 2, width)
    quarter = (chips, PIECES, rows // 2, width // 2)
    dma = pltpu.SemaphoreType.DMA
    meta_shape = (heads + 1 + -(heads + 1) % 8, tok)
    return [
        pltpu.VMEM(meta_shape, F32),
        pltpu.VMEM((tok, 1), F32),
        pltpu.VMEM((others, tok, att), BF16),
        pltpu.VMEM((others, tok, att), BF16),
        pltpu.VMEM((others,) + meta_shape, F32),
        pltpu.VMEM((tok, att), F32),
        pltpu.VMEM((heads, tok, 1), F32),
        pltpu.VMEM(out_weight.shape, BF16),
        pltpu.VMEM((2,) + half, BF16),
        pltpu.VMEM(half, BF16),
        pltpu.VMEM(quarter, BF16),
        pltpu.VMEM(quarter, BF16),
        dma,
        dma((others, 3)),
        dma((others, 3)),
        dma((chips,)),
        dma((chips,)),
    ] + [dma((chips, PIECES))] * 4


def mixer(residual, queries, keys, values, offsets, docs, out_weight, gain):
    heads = offsets.shape[1]
    return pl.pallas_call(
        functools.partial(
            mixer_kernel, lax.axis_size("sp"), lax.axis_size("tp") // 2, heads, (), ()
        ),
        out_shape=[jax.ShapeDtypeStruct(residual.shape, BF16)] * 2,
        in_specs=[VMEM_SPEC] * 7 + [ANY_SPEC],
        out_specs=[VMEM_SPEC] * 2,
        scratch_shapes=mixer_scratch(residual, queries, heads, out_weight),
        compiler_params=pltpu.CompilerParams(
            collective_id=0, has_side_effects=True, vmem_limit_bytes=48 << 20
        ),
        name="mixer",
    )(queries, keys, values, offsets.T, docs[None, :], residual, gain[None, :], out_weight)


def slot_row(ids, tp, rows):
    tok = ids.shape[1]
    group = jnp.broadcast_to((ids[:1, :] // 2).astype(F32), (8, tok)).astype(BF16)
    at = lax.broadcasted_iota(jnp.int32, (tok, 128), 0)
    lane = lax.broadcasted_iota(jnp.int32, (tok, 128), 1)
    pick = jnp.where(at == lane + tp * rows, 1.0, 0.0).astype(BF16)
    mine = jnp.dot(group, pick, preferred_element_type=F32)
    before_at = lax.broadcasted_iota(jnp.int32, (128, 128), 0)
    before_lane = lax.broadcasted_iota(jnp.int32, (128, 128), 1)
    before = jnp.where(before_at < before_lane, 1.0, 0.0).astype(BF16)
    ones = jnp.dot(mine.astype(BF16), before, preferred_element_type=F32)
    token = lax.broadcasted_iota(jnp.int32, (8, 128), 1).astype(F32)
    slot = jnp.where(mine > 0.5, ones + rows // 2, token - ones)
    return slot[:1, :rows]


def experts_kernel(
    chips,
    w_copies,
    normed_ref, mixed_ref, ids_ref, group_ref, expert_ref,
    out_ref,
    router_ref, gate, up, down, rows, y_out, part, partner_in, x_in, down_in, up_in, y_in, total,
    y_sem, rows_recv, line_send, x_send, fan_send,
    p_send, p_recv, xr_send, xr_recv, down_send, down_recv, up_send, up_recv,
):
    sp = lax.axis_index("sp")
    tp = lax.axis_index("tp")
    y, x = sp // 2, sp % 2
    chip, core = tp // 2, tp % 2
    partner = (sp, tp + 1 - 2 * core)
    x_peer = (sp + 1 - 2 * x, tp)
    y_peer = (lax.rem(sp + 2, 4), tp)
    below, above = (sp, tp - 2), (sp, tp + 2)
    has_below, has_above = chip > 0, chip < chips - 1
    half_rows, width = rows.shape[4:]

    row_count = 2 * half_rows
    slots = slot_row(ids_ref[...], tp, row_count)
    slot_iota = lax.broadcasted_iota(jnp.int32, (half_rows, row_count), 0)

    def selection(group):
        wanted = (slot_iota + group * half_rows).astype(F32)
        return jnp.where(wanted == slots, 1.0, 0.0).astype(BF16)

    sel_own, sel_other = selection(y), selection(1 - y)
    router_ref[...] = jnp.zeros_like(router_ref)
    router_ref[0:2, :] = group_ref[...].astype(F32)
    router_ref[2:6, :] = expert_ref[...].astype(F32)
    own = jnp.dot(sel_own, normed_ref[...], preferred_element_type=F32).astype(BF16)
    other = jnp.dot(sel_other, normed_ref[...], preferred_element_type=F32).astype(BF16)
    rows[x, chip, core, y] = own
    y_out[...] = other

    y_copy = remote(
        y_out, rows.at[x, chip, core, y], y_sem.at[0], rows_recv.at[x, chip, core, y], y_peer
    )
    y_copy.start()

    def piece_copy(xs, z, c, s, send, device):
        piece = rows.at[xs, z, c, s]
        return remote(piece, piece, send, rows_recv.at[xs, z, c, s], device)

    def line_piece(z, s, up_ok, down_ok, act):
        @pl.when(down_ok)
        def _():
            act(piece_copy(x, z, core, s, line_send.at[z, s, 0], below))

        @pl.when(up_ok)
        def _():
            act(piece_copy(x, z, core, s, line_send.at[z, s, 1], above))

        act(piece_copy(x, z, core, s, x_send.at[z, s], x_peer))
        act(piece_copy(x, z, core, s, fan_send.at[0, z, s], partner))

    def begin(copy):
        copy.start()

    def arrived(xs, z, c, s):
        piece_copy(xs, z, c, s, y_sem.at[0], x_peer).wait_recv()

    def own_pieces(act, wait):
        line_piece(chip, y, has_above, has_below, act)
        if wait:
            arrived(x, chip, core, 1 - y)
        line_piece(chip, 1 - y, has_above, has_below, act)

    def line_pieces(distance, act, wait):
        for turn in range(2):
            s = y if turn == 0 else 1 - y

            @pl.when(chip - distance >= 0)
            def _():
                if wait:
                    arrived(x, chip - distance, core, s)
                line_piece(chip - distance, s, has_above, chip < 0, act)

            @pl.when(chip + distance < chips)
            def _():
                if wait:
                    arrived(x, chip + distance, core, s)
                line_piece(chip + distance, s, chip < 0, has_below, act)

    def at_distance(distance, body):
        if distance == 0:
            body(chip)
            return

        @pl.when(chip - distance >= 0)
        def _():
            body(chip - distance)

        @pl.when(chip + distance < chips)
        def _():
            body(chip + distance)

    def cross(z, act, wait):
        for turn in range(2):
            s = y if turn == 0 else 1 - y
            if wait:
                arrived(1 - x, z, core, s)
            act(piece_copy(1 - x, z, core, s, fan_send.at[1, z, s], partner))

    def p_copy(z):
        return remote(part.at[z, 1 - core], partner_in.at[z], p_send.at[z], p_recv.at[z], partner)

    def xr_copy(z, s):
        return remote(
            part.at[z, core, 1 - x, s], x_in.at[z, s], xr_send.at[z, s], xr_recv.at[z, s], x_peer
        )

    lanes = lax.broadcasted_iota(jnp.int32, (1, router_ref.shape[0]), 1)

    def signed(plus, minus):
        return jnp.where(lanes == plus, 1.0, 0.0) - jnp.where(lanes == minus, 1.0, 0.0)

    group_sign = signed(y, 1 - y)
    expert_sign = signed(2 + sp, 2 + sp + 1 - 2 * x)

    def expert(z):
        for xs in range(2):
            for s in range(2):
                arrived(xs, z, 1 - core, s)
        block = rows[:, z].reshape(8 * half_rows, width)
        logits = lax.dot_general(
            block, router_ref[...].astype(BF16), (((1,), (1,)), ((), ())), preferred_element_type=F32
        )
        route = jax.nn.sigmoid(
            jnp.sum(logits * group_sign, axis=1, keepdims=True)
        ) * jax.nn.sigmoid(jnp.sum(logits * expert_sign, axis=1, keepdims=True))
        gated = jnp.dot(block, gate[...], preferred_element_type=F32)
        raised = jnp.dot(block, up[...], preferred_element_type=F32)
        hidden = (jax.nn.silu(gated) * raised).astype(BF16)
        tile = 1024
        for n in range(width // tile):
            cols = slice(n * tile, (n + 1) * tile)
            out = jnp.dot(hidden, down[:, cols], preferred_element_type=F32) * route
            out = out.astype(BF16)
            for xs in range(2):
                for c in range(2):
                    for s in range(2):
                        at = ((xs * 2 + c) * 2 + s) * half_rows
                        part[z, c, xs, s, :, cols] = out[at : at + half_rows]
        p_copy(z).start()

    halves = (1 - y, y)

    def join_cores(z, send=True):
        p_copy(z).wait_recv()
        for xs in (1 - x, x):
            for s in halves:
                part[z, core, xs, s] = (
                    part[z, core, xs, s].astype(F32) + partner_in[z, xs, s].astype(F32)
                ).astype(BF16)
                if xs is not x and send:
                    xr_copy(z, s).start()

    def join_x(z, piece):
        s = halves[piece // 2]
        if piece % 2 == 0:
            xr_copy(z, s).wait_recv()
            part[z, core, x, s] = (
                part[z, core, x, s].astype(F32) + x_in[z, s].astype(F32)
            ).astype(BF16)

    def back_copy(n):
        cols = columns(n, width)
        return remote(
            part.at[chip, core, x, 1 - y, :, cols], y_in.at[:, cols], y_sem.at[1 + n],
            y_sem.at[3 + n], y_peer,
        )

    def finished(piece):
        cols = columns(piece, width)
        if piece < 2:
            back_copy(piece).start()
        else:
            sums = lax.dot_general(
                sel_own, part[chip, core, x, y, :, cols], (((0,), (0,)), ((), ())),
                preferred_element_type=F32,
            )
            total[:, cols] = mixed_ref[:, cols].astype(F32) + sums

    own_pieces(begin, True)
    for distance in range(1, chips + 1):
        if distance < chips:
            line_pieces(distance, begin, True)
        at_distance(distance - 1, lambda z: cross(z, begin, True))
        if distance == 1:
            for copy in w_copies:
                copy.wait()
        at_distance(distance - 1, expert)
        if distance > 1:
            at_distance(distance - 2, lambda z: join_cores(z, distance > 2))
    at_distance(chips - 1, join_cores)
    for s in halves:
        xr_copy(chip, s).start()
    finish = line_reduce(
        chips, chip, sp, tp,
        lambda z, p: part.at[z, core, x, halves[p // 2], :, columns(p, width)],
        down_in, up_in, (down_send, down_recv, up_send, up_recv), join_x, finished, True,
    )
    for n in range(2):
        cols = columns(n, width)
        back_copy(n).wait_recv()
        sums = lax.dot_general(
            sel_other, y_in[:, cols], (((0,), (0,)), ((), ())), preferred_element_type=F32
        )
        out_ref[:, cols] = (total[:, cols] + sums).astype(BF16)

    def end(copy):
        copy.wait_send()

    for n in range(2):
        back_copy(n).wait_send()
    y_copy.wait_send()
    own_pieces(end, False)
    for distance in range(chips):
        if distance:
            line_pieces(distance, end, False)
        at_distance(distance, lambda z: cross(z, end, False))
        at_distance(distance, lambda z: end(p_copy(z)))
        for s in range(2):
            at_distance(distance, lambda z: end(xr_copy(z, s)))
    finish()


def layer_kernel(
    sp_count, chips, heads, mixer_count,
    q_hbm, k_hbm, v_hbm, res_hbm, w_hbm, gate_hbm, up_hbm, down_hbm,
    off_ref, doc_ref, gain_ref, ids_ref, group_ref, expert_ref,
    out_ref,
    q_ref, k_ref, v_ref, res_ref, mixed_ref, normed_ref, load_sem, weight_sem, router_ref,
    gate, up, down,
    *scratch,
):
    loads = [
        pltpu.make_async_copy(src, dst, load_sem.at[n])
        for n, (src, dst) in enumerate(
            ((k_hbm, k_ref), (v_hbm, v_ref), (q_hbm, q_ref), (res_hbm, res_ref))
        )
    ]
    weights = [
        pltpu.make_async_copy(src.at[0], dst, weight_sem.at[n])
        for n, (src, dst) in enumerate(((gate_hbm, gate), (up_hbm, up), (down_hbm, down)))
    ]
    for copy in loads[:3]:
        copy.start()
    mixer_kernel(
        sp_count, chips, heads, loads[:3], loads[3:] + weights,
        q_ref, k_ref, v_ref, off_ref, doc_ref, res_ref, gain_ref, w_hbm,
        mixed_ref, normed_ref, *scratch[:mixer_count],
    )
    experts_kernel(
        chips, weights, normed_ref, mixed_ref, ids_ref, group_ref, expert_ref, out_ref,
        router_ref, gate, up, down, *scratch[mixer_count:],
    )


def pair_layer(
    residual, queries, keys, values, offsets, docs, out_weight, gain,
    expert_ids, group_router, expert_router, gate, up, down,
):
    chips = lax.axis_size("tp") // 2
    rows, width = residual.shape
    heads = offsets.shape[1]
    mixer_parts = mixer_scratch(residual, queries, heads, out_weight)
    half_rows = rows // 2
    units = gate.shape[2]
    half = (chips, 2, half_rows, width)
    quarter = (chips, PIECES, half_rows, width // 2)
    dma = pltpu.SemaphoreType.DMA
    return pl.pallas_call(
        functools.partial(
            layer_kernel, lax.axis_size("sp"), chips, heads, len(mixer_parts)
        ),
        out_shape=jax.ShapeDtypeStruct((rows, width), BF16),
        in_specs=[ANY_SPEC] * 8 + [VMEM_SPEC] * 6,
        out_specs=VMEM_SPEC,
        scratch_shapes=[
            pltpu.VMEM(queries.shape, BF16),
            pltpu.VMEM(keys.shape, BF16),
            pltpu.VMEM(values.shape, BF16),
            pltpu.VMEM((rows, width), BF16),
            pltpu.VMEM((rows, width), BF16),
            pltpu.VMEM((rows, width), BF16),
            dma((4,)),
            dma((3,)),
            pltpu.VMEM((8, width), F32),
            pltpu.VMEM((width, units), BF16),
            pltpu.VMEM((width, units), BF16),
            pltpu.VMEM((units, width), BF16),
        ]
        + mixer_parts
        + [
            pltpu.VMEM((2, chips, 2, 2, half_rows, width), BF16),
            pltpu.VMEM((half_rows, width), BF16),
            pltpu.VMEM((chips, 2, 2, 2, half_rows, width), BF16),
            pltpu.VMEM((chips, 2, 2, half_rows, width), BF16),
            pltpu.VMEM(half, BF16),
            pltpu.VMEM(quarter, BF16),
            pltpu.VMEM(quarter, BF16),
            pltpu.VMEM((half_rows, width), BF16),
            pltpu.VMEM((rows, width), F32),
            dma((5,)),
            dma((2, chips, 2, 2)),
            dma((chips, 2, 2)),
            dma((chips, 2)),
            dma((2, chips, 2)),
            dma((chips,)),
            dma((chips,)),
            dma((chips, 2)),
            dma((chips, 2)),
        ]
        + [dma((chips, PIECES))] * 4,
        compiler_params=pltpu.CompilerParams(
            collective_id=1, has_side_effects=True, vmem_limit_bytes=60 << 20
        ),
        name="layer",
    )(
        queries, keys, values, residual, out_weight, gate, up, down,
        offsets.T, docs[None, :], gain[None, :], expert_ids.T, group_router.T, expert_router.T,
    )


def per_device(
    residual_in,
    queries,
    keys,
    values,
    break_offset,
    doc_ids,
    out_weight,
    norm_gain,
    group_router,
    expert_router,
    expert_ids,
    gate_weight,
    up_weight,
    down_weight,
):
    tok_dev = queries.shape[0]
    sp_count = lax.axis_size("sp")
    tp_count = lax.axis_size("tp")
    tp_rank = lax.axis_index("tp")
    width = residual_in.shape[1]
    rows_dev = tok_dev // tp_count
    chosen = lax.dynamic_slice_in_dim(expert_ids, tp_rank * rows_dev, rows_dev, 0)
    expert_count = sp_count * gate_weight.shape[0]
    group_size = expert_count // GROUPS
    if sp_count == 4 and gate_weight.shape[0] == 1 and rows_dev % 32 == 0:
        return pair_layer(
            residual_in, queries, keys, values, break_offset, doc_ids, out_weight, norm_gain,
            expert_ids, group_router, expert_router, gate_weight, up_weight, down_weight,
        )
    mixed_stream, normed = mixer(
        residual_in, queries, keys, values, break_offset, doc_ids, out_weight, norm_gain
    )
    routes = route_weights(normed, group_router, expert_router, chosen, group_size)
    slots = 2 * rows_dev // expert_count
    slot_ids = slot_table(chosen, expert_count, slots)
    sent = dispatch(normed, slot_ids, expert_count * slots).reshape(expert_count, slots, width)
    fanned = lax.all_gather(
        lax.all_to_all(sent, "sp", split_axis=0, concat_axis=0, tiled=True),
        "tp",
        axis=0,
        tiled=True,
    )
    partial_out = expert_rows(
        fanned.reshape(-1, width), gate_weight[0], up_weight[0], down_weight[0]
    )
    unit_total = lax.psum_scatter(
        partial_out.reshape(fanned.shape), "tp", scatter_dimension=0, tiled=True
    ).astype(jnp.float32)
    returned = lax.all_to_all(
        unit_total.astype(jnp.bfloat16), "sp", split_axis=0, concat_axis=0, tiled=True
    )
    expert_out = jnp.take(returned.reshape(-1, width), slot_ids.reshape(-1), axis=0).reshape(
        rows_dev, 2, width
    )
    mixture = jnp.sum(routes[:, :, None] * expert_out.astype(jnp.float32), axis=1)
    return (mixed_stream.astype(jnp.float32) + mixture).astype(jnp.bfloat16)


def solution(mesh):
    return jax.shard_map(
        per_device,
        mesh=mesh,
        in_specs=(
            P(("sp", "tp"), None),
            P("sp", "tp"),
            P("sp", "tp"),
            P("sp", "tp"),
            P("sp", "tp"),
            P("sp"),
            P("tp", None),
            P(),
            P(),
            P(),
            P("sp", None),
            P("sp", None, "tp"),
            P("sp", None, "tp"),
            P("sp", "tp", None),
        ),
        out_specs=P(("sp", "tp"), None),
        check_vma=False,
    )
```

```python
import functools

import jax
import jax.numpy as jnp
from jax import lax
from jax.experimental import pallas as pl
from jax.experimental.pallas import tpu as pltpu
from jax.sharding import PartitionSpec as P

HEAD_DIM = 64
PIECES = 4
GROUPS = 2


def route_weights(normed, group_router, expert_router, chosen, group_size):
    group_logits = jnp.dot(normed, group_router, preferred_element_type=jnp.float32)
    expert_logits = jnp.dot(normed, expert_router, preferred_element_type=jnp.float32)
    chosen_group = chosen[:, 0] // group_size
    margin = group_logits[:, 0] - group_logits[:, 1]
    own_margin = jnp.where(chosen_group == 0, margin, -margin)
    experts_iota = jnp.arange(expert_logits.shape[1], dtype=jnp.int32)
    picked = jnp.sum(
        jnp.where(
            chosen[:, :, None] == experts_iota[None, None, :],
            expert_logits[:, None, :],
            jnp.float32(0.0),
        ),
        axis=2,
    )
    return jax.nn.sigmoid(own_margin)[:, None] * jax.nn.sigmoid(picked - picked[:, ::-1])


def slot_table(chosen, expert_count, slots):
    flat_ids = chosen.reshape(-1)
    onehot = (flat_ids[:, None] == jnp.arange(expert_count, dtype=jnp.int32)[None, :]).astype(
        jnp.int32
    )
    before = jnp.cumsum(onehot, axis=0) - onehot
    ranks = jnp.sum(before * onehot, axis=1)
    return (flat_ids * slots + ranks).reshape(chosen.shape)


def dispatch(normed, slot_ids, total_slots):
    flat_slots = slot_ids.reshape(-1)
    owners = jnp.arange(flat_slots.shape[0], dtype=jnp.int32) // 2
    slot_iota = jnp.arange(total_slots, dtype=jnp.int32)
    token_of_slot = jnp.sum(
        jnp.where(slot_iota[:, None] == flat_slots[None, :], owners[None, :], 0), axis=1
    )
    return jnp.take(normed, token_of_slot, axis=0)


def expert_rows(row_block, gate_part, up_part, down_part):
    gate_val = jnp.dot(row_block, gate_part, preferred_element_type=jnp.float32)
    up_val = jnp.dot(row_block, up_part, preferred_element_type=jnp.float32)
    hidden = (jax.nn.silu(gate_val) * up_val).astype(jnp.bfloat16)
    return jnp.dot(hidden, down_part, preferred_element_type=jnp.float32).astype(jnp.bfloat16)


MESH_ID = pl.DeviceIdType.MESH
VMEM_SPEC = pl.BlockSpec(memory_space=pltpu.VMEM)
ANY_SPEC = pl.BlockSpec(memory_space=pl.ANY)
F32 = jnp.float32
BF16 = jnp.bfloat16


def remote(src, dst, send_sem, recv_sem, device):
    return pltpu.make_async_remote_copy(
        src_ref=src, dst_ref=dst, send_sem=send_sem, recv_sem=recv_sem,
        device_id=device, device_id_type=MESH_ID,
    )


def columns(piece, width):
    return pl.ds((piece % 2) * (width // 2), width // 2)


def greet(device):
    pl.semaphore_signal(
        pltpu.get_barrier_semaphore(), inc=1, device_id=device, device_id_type=MESH_ID
    )


class Line:
    def __init__(self, chips, chip, sp, tp, block, down_in, up_in, sems):
        self.chips, self.chip, self.me, self.block = chips, chip, (sp, tp), block
        down_send, down_recv, up_send, up_recv = sems
        self.legs = (
            (down_in, down_send, down_recv, (sp, tp - 2), chip < chips - 1),
            (up_in, up_send, up_recv, (sp, tp + 2), chip > 0),
        )

    def copy(self, leg, dest, p, device):
        inbox, send, recv = leg[:3]
        return remote(
            self.block(dest, p), inbox.at[dest, p], send.at[dest, p], recv.at[dest, p], device
        )

    def gather(self, leg, dest, p, device):
        @pl.when(leg[4])
        def _():
            self.copy(leg, dest, p, device).wait_recv()
            piece = self.block(dest, p)
            piece[...] = (piece[...].astype(F32) + leg[0][dest, p].astype(F32)).astype(BF16)

    def send(self, below, above, pieces, ready):
        chip, chips = self.chip, self.chips
        for p in pieces:
            for leg, dest, valid in (
                (self.legs[0], below, (below >= 0) & (below < chip)),
                (self.legs[1], above, (above > chip) & (above < chips)),
            ):

                @pl.when(valid)
                def _():
                    ready(dest, p)
                    self.gather(leg, dest, p, leg[3])
                    self.copy(leg, dest, p, leg[3]).start()

    def own(self, p, ready):
        ready(self.chip, p)
        for leg in self.legs:
            self.gather(leg, self.chip, p, leg[3])

    def drain(self):
        for dest in range(self.chips):
            for leg, sent in ((self.legs[0], dest < self.chip), (self.legs[1], dest > self.chip)):

                @pl.when(sent)
                def _():
                    for p in range(PIECES):
                        self.copy(leg, dest, p, leg[3]).wait_send()


def attention(
    sp_count, chips, heads, loads, later_loads,
    q_ref, k_ref, v_ref, off_ref, doc_ref,
    meta_ref, doc_col, k_buf, v_buf, m_buf, acc, carry, kv_send, kv_recv,
):
    sp = lax.axis_index("sp")
    tp = lax.axis_index("tp")
    chip = tp // 2
    core = tp % 2
    partner = tp + 1 - 2 * core
    tok, att = q_ref.shape
    for j in range(1, sp_count):
        greet((lax.rem(sp + j, sp_count), tp))
    greet((sp, partner))

    @pl.when(chip > 0)
    def _():
        greet((sp, tp - 2))

    @pl.when(chip < chips - 1)
    def _():
        greet((sp, tp + 2))

    expect = sp_count + jnp.where(chip > 0, 1, 0) + jnp.where(chip < chips - 1, 1, 0)
    docs = doc_ref[...].astype(F32)
    meta_ref[...] = jnp.zeros_like(meta_ref)
    meta_ref[0:heads, :] = off_ref[...].astype(F32)
    meta_ref[heads : heads + 1, :] = docs
    doc_col[...] = jnp.broadcast_to(docs, (128, tok)).T[:, :1]
    for copy in loads:
        copy.wait()
    pl.semaphore_wait(pltpu.get_barrier_semaphore(), expect)

    def kv_copies(j, target):
        return [
            remote(src, buf.at[j - 1], kv_send.at[j - 1, n], kv_recv.at[j - 1, n], (target, tp))
            for n, (src, buf) in enumerate(((k_ref, k_buf), (v_ref, v_buf), (meta_ref, m_buf)))
        ]

    for j in range(1, sp_count):

        @pl.when(sp + j < sp_count)
        def _():
            for copy in kv_copies(j, sp + j):
                copy.start()

    for copy in later_loads:
        copy.start()

    row = lax.broadcasted_iota(jnp.int32, (tok, tok), 0)
    col = lax.broadcasted_iota(jnp.int32, (tok, tok), 1)
    later = jnp.where(row > col, 1.0, 0.0).astype(BF16)
    lane = lax.broadcasted_iota(jnp.int32, (tok, att), 1) // HEAD_DIM
    acc[...] = jnp.zeros_like(acc)
    carry[...] = jnp.zeros_like(carry)

    def attend_block(keys, vals, meta, own):
        live = doc_col[...] == meta[heads : heads + 1, :]
        if own:
            live = live & (col < row)
        for h in range(heads):
            queries = jnp.where(lane == h, q_ref[...], jnp.zeros((), BF16)) * jnp.asarray(
                HEAD_DIM ** (-0.5), BF16
            )
            scores = lax.dot_general(
                queries, keys, (((1,), (1,)), ((), ())), preferred_element_type=F32
            ) + meta[h : h + 1, :]
            soft = jnp.maximum(scores, 0.0) + jnp.log(1.0 + jnp.exp(-jnp.abs(scores)))
            stay = jnp.where(live, -soft, 0.0)
            high = stay.astype(BF16)
            low = (stay - high.astype(F32)).astype(BF16)
            within = jnp.dot(high, later, preferred_element_type=F32) + jnp.dot(
                low, later, preferred_element_type=F32
            )
            before = carry[h]
            weights = jnp.where(
                live, jnp.exp(scores - soft + within + before), 0.0
            ).astype(BF16)
            out = jnp.dot(weights, vals, preferred_element_type=F32)
            acc[...] += jnp.where(lane == h, out, 0.0)
            carry[h] = before + within[:, :1] + stay[:, :1]

    attend_block(k_ref[...], v_ref[...], meta_ref[...], True)

    def earlier(j, unused):
        @pl.when(sp - j >= 0)
        def _():
            for copy in kv_copies(j, sp):
                copy.wait_recv()
            attend_block(k_buf[j - 1], v_buf[j - 1], m_buf[j - 1], False)

        return unused

    lax.fori_loop(1, sp_count, earlier, 0)
    for j in range(1, sp_count):

        @pl.when(sp + j < sp_count)
        def _():
            for copy in kv_copies(j, sp + j):
                copy.wait_send()

    return acc[...].astype(BF16)


def project(attended, w_buf, part, chips, half_rows, first, last):
    tile = 512
    for n in range(first // tile, last // tile):
        cols = slice(n * tile, (n + 1) * tile)
        product = jnp.dot(attended, w_buf[:, cols], preferred_element_type=F32).astype(BF16)
        for z in range(chips):
            for c in range(2):
                for s in range(2):
                    at = ((z * 2 + c) * 2 + s) * half_rows
                    part[c, z, s, :, cols] = product[at : at + half_rows]


def mixer_kernel(
    sp_count, chips, heads,
    q_ref, k_ref, v_ref, off_ref, doc_ref, res_ref, gain_ref, w_hbm,
    mixed_ref, normed_ref,
    meta_ref, doc_col, k_buf, v_buf, m_buf, acc, carry, w_buf, part, partner_in, down_in, up_in,
    w_sem, kv_send, kv_recv, p_send, p_recv, down_send, down_recv, up_send, up_recv,
):
    sp = lax.axis_index("sp")
    tp = lax.axis_index("tp")
    chip = tp // 2
    core = tp % 2
    width = res_ref.shape[1]
    half_rows = res_ref.shape[0] // 2
    w_copy = pltpu.make_async_copy(w_hbm, w_buf, w_sem)
    attended = attention(
        sp_count, chips, heads, (), (w_copy,),
        q_ref, k_ref, v_ref, off_ref, doc_ref,
        meta_ref, doc_col, k_buf, v_buf, m_buf, acc, carry, kv_send, kv_recv,
    )
    w_copy.wait()
    project(attended, w_buf, part, chips, half_rows, 0, width)

    def p_copy(z):
        return remote(
            part.at[1 - core, z], partner_in.at[z], p_send.at[z, 0], p_recv.at[z, 0],
            (sp, tp + 1 - 2 * core),
        )

    for z in range(chips):
        p_copy(z).start()
    for z in range(chips):
        p_copy(z).wait_recv()
        part[core, z] = (part[core, z].astype(F32) + partner_in[z].astype(F32)).astype(BF16)
    line = Line(
        chips, chip, sp, tp, lambda z, p: part.at[core, z, p // 2, :, columns(p, width)],
        down_in, up_in, (down_send, down_recv, up_send, up_recv),
    )
    for distance in range(chips - 1, 0, -1):
        line.send(chip - distance, chip + distance, range(PIECES), lambda dest, p: None)
    for p in range(PIECES):
        line.own(p, lambda dest, p: None)
    total = part[core, chip].reshape(res_ref.shape).astype(F32)
    mixed = (res_ref[...].astype(F32) + total).astype(BF16)
    mixed_ref[...] = mixed
    mixed_f = mixed.astype(F32)
    scaling = lax.rsqrt(jnp.mean(mixed_f * mixed_f, axis=1, keepdims=True) + 1e-06)
    normed_ref[...] = (mixed_f * scaling * gain_ref[...]).astype(BF16)
    for z in range(chips):
        p_copy(z).wait_send()
    line.drain()


def mixer_scratch(residual, queries, heads, out_weight):
    sp_count = lax.axis_size("sp")
    chips = lax.axis_size("tp") // 2
    rows, width = residual.shape
    tok, att = queries.shape
    others = max(sp_count - 1, 1)
    half = (chips, 2, rows // 2, width)
    quarter = (chips, PIECES, rows // 2, width // 2)
    dma = pltpu.SemaphoreType.DMA
    meta_shape = (heads + 1 + -(heads + 1) % 8, tok)
    return [
        pltpu.VMEM(meta_shape, F32),
        pltpu.VMEM((tok, 1), F32),
        pltpu.VMEM((others, tok, att), BF16),
        pltpu.VMEM((others, tok, att), BF16),
        pltpu.VMEM((others,) + meta_shape, F32),
        pltpu.VMEM((tok, att), F32),
        pltpu.VMEM((heads, tok, 1), F32),
        pltpu.VMEM(out_weight.shape, BF16),
        pltpu.VMEM((2,) + half, BF16),
        pltpu.VMEM(half, BF16),
        pltpu.VMEM(quarter, BF16),
        pltpu.VMEM(quarter, BF16),
        dma,
        dma((others, 3)),
        dma((others, 3)),
        dma((chips, 2)),
        dma((chips, 2)),
    ] + [dma((chips, PIECES))] * 4


def mixer(residual, queries, keys, values, offsets, docs, out_weight, gain):
    heads = offsets.shape[1]
    return pl.pallas_call(
        functools.partial(
            mixer_kernel, lax.axis_size("sp"), lax.axis_size("tp") // 2, heads
        ),
        out_shape=[jax.ShapeDtypeStruct(residual.shape, BF16)] * 2,
        in_specs=[VMEM_SPEC] * 7 + [ANY_SPEC],
        out_specs=[VMEM_SPEC] * 2,
        scratch_shapes=mixer_scratch(residual, queries, heads, out_weight),
        compiler_params=pltpu.CompilerParams(
            collective_id=0, has_side_effects=True, vmem_limit_bytes=48 << 20
        ),
        name="mixer",
    )(queries, keys, values, offsets.T, docs[None, :], residual, gain[None, :], out_weight)


def slot_row(ids, tp, rows):
    tok = ids.shape[1]
    group = jnp.broadcast_to((ids[:1, :] // 2).astype(F32), (8, tok)).astype(BF16)
    at = lax.broadcasted_iota(jnp.int32, (tok, 128), 0)
    lane = lax.broadcasted_iota(jnp.int32, (tok, 128), 1)
    pick = jnp.where(at == lane + tp * rows, 1.0, 0.0).astype(BF16)
    mine = jnp.dot(group, pick, preferred_element_type=F32)
    before_at = lax.broadcasted_iota(jnp.int32, (128, 128), 0)
    before_lane = lax.broadcasted_iota(jnp.int32, (128, 128), 1)
    before = jnp.where(before_at < before_lane, 1.0, 0.0).astype(BF16)
    ones = jnp.dot(mine.astype(BF16), before, preferred_element_type=F32)
    token = lax.broadcasted_iota(jnp.int32, (8, 128), 1).astype(F32)
    slot = jnp.where(mine > 0.5, ones + rows // 2, token - ones)
    return slot[:1, :rows]


def experts_kernel(
    chips,
    w_copies, w_copy, res_copy, attended,
    mixed_ref, res_ref, gain_ref, ids_ref, group_ref, expert_ref,
    out_ref,
    w_buf, sums, sums_in, a_down_in, a_up_in, a_send, a_recv, a_sems,
    router_ref, gate, up, down, rows, y_out, part, partner_in, x_in, down_in, up_in, y_in, total,
    y_sem, rows_recv, line_send, x_send, fan_send,
    p_send, p_recv, xr_send, xr_recv, down_send, down_recv, up_send, up_recv,
):
    sp = lax.axis_index("sp")
    tp = lax.axis_index("tp")
    y, x = sp // 2, sp % 2
    chip, core = tp // 2, tp % 2
    partner = (sp, tp + 1 - 2 * core)
    x_peer = (sp + 1 - 2 * x, tp)
    y_peer = (lax.rem(sp + 2, 4), tp)
    below, above = (sp, tp - 2), (sp, tp + 2)
    has_below, has_above = chip > 0, chip < chips - 1
    row_count, width = res_ref.shape
    half_rows = row_count // 2
    half_width = width // 2

    slots = slot_row(ids_ref[...], tp, row_count)
    slot_iota = lax.broadcasted_iota(jnp.int32, (half_rows, row_count), 0)

    def selection(group):
        wanted = (slot_iota + group * half_rows).astype(F32)
        return jnp.where(wanted == slots, 1.0, 0.0).astype(BF16)

    sel_own, sel_other = selection(y), selection(1 - y)
    router_ref[...] = jnp.zeros_like(router_ref)
    router_ref[0:2, :] = group_ref[...].astype(F32)
    router_ref[2:6, :] = expert_ref[...].astype(F32)

    def span(h):
        return pl.ds(h * half_width, half_width + (rows.shape[5] - width) * h)

    def y_copy(h):
        return remote(
            y_out.at[:, span(h)], rows.at[x, chip, core, y, :, span(h)], y_sem.at[5 + h],
            rows_recv.at[x, chip, core, y, h], y_peer,
        )

    def piece_copy(xs, z, c, s, h, send, device):
        piece = rows.at[xs, z, c, s, :, span(h)]
        return remote(piece, piece, send, rows_recv.at[xs, z, c, s, h], device)

    def line_piece(z, s, h, up_ok, down_ok, act):
        @pl.when(down_ok)
        def _():
            act(piece_copy(x, z, core, s, h, line_send.at[z, s, 0, h], below))

        @pl.when(up_ok)
        def _():
            act(piece_copy(x, z, core, s, h, line_send.at[z, s, 1, h], above))

        act(piece_copy(x, z, core, s, h, x_send.at[z, s, h], x_peer))
        act(piece_copy(x, z, core, s, h, fan_send.at[0, z, s, h], partner))

    def begin(copy):
        copy.start()

    def arrived(xs, z, c, s, h):
        piece_copy(xs, z, c, s, h, y_sem.at[0], x_peer).wait_recv()

    def own_rest(h):
        arrived(x, chip, core, 1 - y, h)
        line_piece(chip, 1 - y, h, has_above, has_below, begin)

    def line_pieces(distance, h, act, wait):
        for turn in range(2):
            s = y if turn == 0 else 1 - y

            @pl.when(chip - distance >= 0)
            def _():
                if wait:
                    arrived(x, chip - distance, core, s, h)
                line_piece(chip - distance, s, h, has_above, chip < 0, act)

            @pl.when(chip + distance < chips)
            def _():
                if wait:
                    arrived(x, chip + distance, core, s, h)
                line_piece(chip + distance, s, h, chip < 0, has_below, act)

    def at_distance(distance, body):
        if distance == 0:
            body(chip)
            return

        @pl.when(chip - distance >= 0)
        def _():
            body(chip - distance)

        @pl.when(chip + distance < chips)
        def _():
            body(chip + distance)

    def cross(z, h, act, wait):
        for turn in range(2):
            s = y if turn == 0 else 1 - y
            if wait:
                arrived(1 - x, z, core, s, h)
            act(piece_copy(1 - x, z, core, s, h, fan_send.at[1, z, s, h], partner))

    def a_copy(z, h):
        cols = columns(h, width)
        return remote(
            sums.at[1 - core, z, :, :, cols], sums_in.at[z, :, :, cols], a_send.at[z, h],
            a_recv.at[z, h], partner,
        )

    w_copy.wait()
    for h in range(2):
        project(attended, w_buf, sums, chips, half_rows, h * half_width, (h + 1) * half_width)
        for z in range(chips):
            a_copy(z, h).start()

    def fold(dest, p):
        if p < 2:
            cols = columns(p, width)
            a_copy(dest, p).wait_recv()
            sums[core, dest, :, :, cols] = (
                sums[core, dest, :, :, cols].astype(F32) + sums_in[dest, :, :, cols].astype(F32)
            ).astype(BF16)

    mix = Line(
        chips, chip, sp, tp, lambda z, p: sums.at[core, z, p // 2, :, columns(p, width)],
        a_down_in, a_up_in, a_sems,
    )

    def mix_turn(distance, h):
        mix.send(chip - distance, chip + distance, (h, 2 + h), fold)

    squares = []

    def settle(h):
        for p in (h, 2 + h):
            mix.own(p, fold)
        cols = columns(h, width)
        added = sums[core, chip, :, :, cols].reshape(row_count, half_width).astype(F32)
        mixed = (res_ref[:, cols].astype(F32) + added).astype(BF16)
        mixed_ref[:, cols] = mixed
        mixed_f = mixed.astype(F32)
        squares.append(jnp.sum(mixed_f * mixed_f, axis=1, keepdims=True))
        scaled = (mixed_f * gain_ref[:, cols]).astype(BF16)

        def put(group_sel, target):
            target[:, pl.ds(h * half_width, half_width)] = jnp.dot(
                group_sel, scaled, preferred_element_type=F32
            ).astype(BF16)

        own_rows = rows.at[x, chip, core, y]
        put(sel_other, y_out)
        put(sel_own, own_rows)
        if h == 1:
            factor = lax.rsqrt((squares[0] + squares[1]) * (1.0 / width) + 1e-06)
            high = factor.astype(BF16).astype(F32)
            middle = (factor - high).astype(BF16).astype(F32)
            low = factor - high - middle
            lane = lax.broadcasted_iota(jnp.int32, (row_count, 128), 1)
            terms = jnp.where(
                lane == 0, high, jnp.where(lane == 1, middle, jnp.where(lane == 2, low, 0.0))
            ).astype(BF16)
            for group_sel, target in ((sel_other, y_out), (sel_own, own_rows)):
                target[:, pl.ds(width, 128)] = jnp.dot(
                    group_sel, terms, preferred_element_type=F32
                ).astype(BF16)
        y_copy(h).start()
        line_piece(chip, y, h, has_above, has_below, begin)

    def p_copy(z):
        return remote(part.at[z, 1 - core], partner_in.at[z], p_send.at[z], p_recv.at[z], partner)

    def xr_copy(z, s):
        return remote(
            part.at[z, core, 1 - x, s], x_in.at[z, s], xr_send.at[z, s], xr_recv.at[z, s], x_peer
        )

    lanes = lax.broadcasted_iota(jnp.int32, (1, router_ref.shape[0]), 1)

    def signed(plus, minus):
        return jnp.where(lanes == plus, 1.0, 0.0) - jnp.where(lanes == minus, 1.0, 0.0)

    group_sign = signed(y, 1 - y)
    expert_sign = signed(2 + sp, 2 + sp + 1 - 2 * x)

    def expert(z):
        for h in range(2):
            for xs in range(2):
                for s in range(2):
                    arrived(xs, z, 1 - core, s, h)
        block = rows[:, z, :, :, :, :width].reshape(8 * half_rows, width)
        terms = rows[:, z, :, :, :, width:].reshape(8 * half_rows, rows.shape[5] - width)
        factor = jnp.sum(terms.astype(F32), axis=1, keepdims=True)
        logits = lax.dot_general(
            block, router_ref[...].astype(BF16), (((1,), (1,)), ((), ())), preferred_element_type=F32
        )
        logits = logits * factor
        route = jax.nn.sigmoid(
            jnp.sum(logits * group_sign, axis=1, keepdims=True)
        ) * jax.nn.sigmoid(jnp.sum(logits * expert_sign, axis=1, keepdims=True))
        gated = jnp.dot(block, gate[...], preferred_element_type=F32) * factor
        raised = jnp.dot(block, up[...], preferred_element_type=F32) * factor
        hidden = (jax.nn.silu(gated) * raised).astype(BF16)
        tile = 1024
        for n in range(width // tile):
            cols = slice(n * tile, (n + 1) * tile)
            out = jnp.dot(hidden, down[:, cols], preferred_element_type=F32) * route
            out = out.astype(BF16)
            for xs in range(2):
                for c in range(2):
                    for s in range(2):
                        at = ((xs * 2 + c) * 2 + s) * half_rows
                        part[z, c, xs, s, :, cols] = out[at : at + half_rows]
        p_copy(z).start()

    halves = (1 - y, y)

    def join_cores(z, send=True):
        p_copy(z).wait_recv()
        for xs in (1 - x, x):
            for s in halves:
                part[z, core, xs, s] = (
                    part[z, core, xs, s].astype(F32) + partner_in[z, xs, s].astype(F32)
                ).astype(BF16)
                if xs is not x and send:
                    xr_copy(z, s).start()

    def join_x(z, piece):
        s = halves[piece // 2]
        if piece % 2 == 0:
            xr_copy(z, s).wait_recv()
            part[z, core, x, s] = (
                part[z, core, x, s].astype(F32) + x_in[z, s].astype(F32)
            ).astype(BF16)

    def back_copy(n):
        cols = columns(n, width)
        return remote(
            part.at[chip, core, x, 1 - y, :, cols], y_in.at[:, cols], y_sem.at[1 + n],
            y_sem.at[3 + n], y_peer,
        )

    def finished(piece):
        cols = columns(piece, width)
        if piece < 2:
            back_copy(piece).start()
        else:
            sums = lax.dot_general(
                sel_own, part[chip, core, x, y, :, cols], (((0,), (0,)), ((), ())),
                preferred_element_type=F32,
            )
            total[:, cols] = mixed_ref[:, cols].astype(F32) + sums

    for distance in range(chips - 1, 0, -1):
        mix_turn(distance, 0)
    mix_turn(chips - 1, 1)
    res_copy.wait()
    settle(0)
    for distance in range(chips - 2, 0, -1):
        mix_turn(distance, 1)
        if distance == chips - 2:
            own_rest(0)
    line_pieces(1, 0, begin, True)
    settle(1)

    def cross_all(distance, h):
        at_distance(distance, lambda z: cross(z, h, begin, True))

    for distance in range(1, chips + 1):
        if distance + 1 < chips:
            line_pieces(distance + 1, 0, begin, True)
        if distance == 1:
            own_rest(1)
            cross_all(0, 0)
        if distance < chips:
            line_pieces(distance, 1, begin, True)
            cross_all(distance, 0)
        cross_all(distance - 1, 1)
        if distance == 1:
            for copy in w_copies:
                copy.wait()
        at_distance(distance - 1, expert)
        if distance > 1:
            at_distance(distance - 2, lambda z: join_cores(z, distance > 2))
    at_distance(chips - 1, join_cores)
    for s in halves:
        xr_copy(chip, s).start()
    back = Line(
        chips, chip, sp, tp,
        lambda z, p: part.at[z, core, x, halves[p // 2], :, columns(p, width)],
        down_in, up_in, (down_send, down_recv, up_send, up_recv),
    )
    for turn in range(1, 2 * chips - 2):
        back.send(2 * (chips - 1) - turn - chip, turn - chip, range(PIECES), join_x)
    for p in range(PIECES):
        back.own(p, join_x)
        finished(p)
    for n in range(2):
        cols = columns(n, width)
        back_copy(n).wait_recv()
        returned = lax.dot_general(
            sel_other, y_in[:, cols], (((0,), (0,)), ((), ())), preferred_element_type=F32
        )
        out_ref[:, cols] = (total[:, cols] + returned).astype(BF16)

    def end(copy):
        copy.wait_send()

    for n in range(2):
        back_copy(n).wait_send()
    for h in range(2):
        y_copy(h).wait_send()
        for s in (y, 1 - y):
            line_piece(chip, s, h, has_above, has_below, end)
        for distance in range(chips):
            if distance:
                line_pieces(distance, h, end, False)
            at_distance(distance, lambda z: cross(z, h, end, False))
        for z in range(chips):
            end(a_copy(z, h))
    for z in range(chips):
        end(p_copy(z))
        for s in range(2):
            end(xr_copy(z, s))
    mix.drain()
    back.drain()


def layer_kernel(
    sp_count, chips, heads, mixer_count,
    q_hbm, k_hbm, v_hbm, res_hbm, w_hbm, gate_hbm, up_hbm, down_hbm,
    off_ref, doc_ref, gain_ref, ids_ref, group_ref, expert_ref,
    out_ref,
    q_ref, k_ref, v_ref, res_ref, mixed_ref, load_sem, weight_sem, router_ref,
    gate, up, down,
    *scratch,
):
    loads = [
        pltpu.make_async_copy(src, dst, load_sem.at[n])
        for n, (src, dst) in enumerate(
            ((k_hbm, k_ref), (v_hbm, v_ref), (q_hbm, q_ref), (res_hbm, res_ref))
        )
    ]
    weights = [
        pltpu.make_async_copy(src.at[0], dst, weight_sem.at[n])
        for n, (src, dst) in enumerate(((gate_hbm, gate), (up_hbm, up), (down_hbm, down)))
    ]
    for copy in loads[:3]:
        copy.start()
    (
        meta_ref, doc_col, k_buf, v_buf, m_buf, acc, carry, w_buf, sums, sums_in, a_down_in, a_up_in,
        w_sem, kv_send, kv_recv, a_send, a_recv,
    ) = scratch[: mixer_count - 4]
    a_sems = scratch[mixer_count - 4 : mixer_count]
    w_copy = pltpu.make_async_copy(w_hbm, w_buf, w_sem)
    attended = attention(
        sp_count, chips, heads, loads[:3], [w_copy, loads[3]] + weights,
        q_ref, k_ref, v_ref, off_ref, doc_ref,
        meta_ref, doc_col, k_buf, v_buf, m_buf, acc, carry, kv_send, kv_recv,
    )
    experts_kernel(
        chips, weights, w_copy, loads[3], attended,
        mixed_ref, res_ref, gain_ref, ids_ref, group_ref, expert_ref, out_ref,
        w_buf, sums, sums_in, a_down_in, a_up_in, a_send, a_recv, a_sems,
        router_ref, gate, up, down, *scratch[mixer_count:],
    )


def pair_layer(
    residual, queries, keys, values, offsets, docs, out_weight, gain,
    expert_ids, group_router, expert_router, gate, up, down,
):
    chips = lax.axis_size("tp") // 2
    rows, width = residual.shape
    heads = offsets.shape[1]
    mixer_parts = mixer_scratch(residual, queries, heads, out_weight)
    half_rows = rows // 2
    units = gate.shape[2]
    half = (chips, 2, half_rows, width)
    quarter = (chips, PIECES, half_rows, width // 2)
    dma = pltpu.SemaphoreType.DMA
    return pl.pallas_call(
        functools.partial(
            layer_kernel, lax.axis_size("sp"), chips, heads, len(mixer_parts)
        ),
        out_shape=jax.ShapeDtypeStruct((rows, width), BF16),
        in_specs=[ANY_SPEC] * 8 + [VMEM_SPEC] * 6,
        out_specs=VMEM_SPEC,
        scratch_shapes=[
            pltpu.VMEM(queries.shape, BF16),
            pltpu.VMEM(keys.shape, BF16),
            pltpu.VMEM(values.shape, BF16),
            pltpu.VMEM((rows, width), BF16),
            pltpu.VMEM((rows, width), BF16),
            dma((4,)),
            dma((3,)),
            pltpu.VMEM((8, width), F32),
            pltpu.VMEM((width, units), BF16),
            pltpu.VMEM((width, units), BF16),
            pltpu.VMEM((units, width), BF16),
        ]
        + mixer_parts
        + [
            pltpu.VMEM((2, chips, 2, 2, half_rows, width + 128), BF16),
            pltpu.VMEM((half_rows, width + 128), BF16),
            pltpu.VMEM((chips, 2, 2, 2, half_rows, width), BF16),
            pltpu.VMEM((chips, 2, 2, half_rows, width), BF16),
            pltpu.VMEM(half, BF16),
            pltpu.VMEM(quarter, BF16),
            pltpu.VMEM(quarter, BF16),
            pltpu.VMEM((half_rows, width), BF16),
            pltpu.VMEM((rows, width), F32),
            dma((7,)),
            dma((2, chips, 2, 2, 2)),
            dma((chips, 2, 2, 2)),
            dma((chips, 2, 2)),
            dma((2, chips, 2, 2)),
            dma((chips,)),
            dma((chips,)),
            dma((chips, 2)),
            dma((chips, 2)),
        ]
        + [dma((chips, PIECES))] * 4,
        compiler_params=pltpu.CompilerParams(
            collective_id=1, has_side_effects=True, vmem_limit_bytes=60 << 20
        ),
        name="layer",
    )(
        queries, keys, values, residual, out_weight, gate, up, down,
        offsets.T, docs[None, :], gain[None, :], expert_ids.T, group_router.T, expert_router.T,
    )


def per_device(
    residual_in,
    queries,
    keys,
    values,
    break_offset,
    doc_ids,
    out_weight,
    norm_gain,
    group_router,
    expert_router,
    expert_ids,
    gate_weight,
    up_weight,
    down_weight,
):
    tok_dev = queries.shape[0]
    sp_count = lax.axis_size("sp")
    tp_count = lax.axis_size("tp")
    tp_rank = lax.axis_index("tp")
    width = residual_in.shape[1]
    rows_dev = tok_dev // tp_count
    chosen = lax.dynamic_slice_in_dim(expert_ids, tp_rank * rows_dev, rows_dev, 0)
    expert_count = sp_count * gate_weight.shape[0]
    group_size = expert_count // GROUPS
    if sp_count == 4 and gate_weight.shape[0] == 1 and rows_dev % 32 == 0:
        return pair_layer(
            residual_in, queries, keys, values, break_offset, doc_ids, out_weight, norm_gain,
            expert_ids, group_router, expert_router, gate_weight, up_weight, down_weight,
        )
    mixed_stream, normed = mixer(
        residual_in, queries, keys, values, break_offset, doc_ids, out_weight, norm_gain
    )
    routes = route_weights(normed, group_router, expert_router, chosen, group_size)
    slots = 2 * rows_dev // expert_count
    slot_ids = slot_table(chosen, expert_count, slots)
    sent = dispatch(normed, slot_ids, expert_count * slots).reshape(expert_count, slots, width)
    fanned = lax.all_gather(
        lax.all_to_all(sent, "sp", split_axis=0, concat_axis=0, tiled=True),
        "tp",
        axis=0,
        tiled=True,
    )
    partial_out = expert_rows(
        fanned.reshape(-1, width), gate_weight[0], up_weight[0], down_weight[0]
    )
    unit_total = lax.psum_scatter(
        partial_out.reshape(fanned.shape), "tp", scatter_dimension=0, tiled=True
    ).astype(jnp.float32)
    returned = lax.all_to_all(
        unit_total.astype(jnp.bfloat16), "sp", split_axis=0, concat_axis=0, tiled=True
    )
    expert_out = jnp.take(returned.reshape(-1, width), slot_ids.reshape(-1), axis=0).reshape(
        rows_dev, 2, width
    )
    mixture = jnp.sum(routes[:, :, None] * expert_out.astype(jnp.float32), axis=1)
    return (mixed_stream.astype(jnp.float32) + mixture).astype(jnp.bfloat16)


def solution(mesh):
    return jax.shard_map(
        per_device,
        mesh=mesh,
        in_specs=(
            P(("sp", "tp"), None),
            P("sp", "tp"),
            P("sp", "tp"),
            P("sp", "tp"),
            P("sp", "tp"),
            P("sp"),
            P("tp", None),
            P(),
            P(),
            P(),
            P("sp", None),
            P("sp", None, "tp"),
            P("sp", None, "tp"),
            P("sp", "tp", None),
        ),
        out_specs=P(("sp", "tp"), None),
        check_vma=False,
    )
```

```python
import functools

import jax
import jax.numpy as jnp
from jax import lax
from jax.experimental import pallas as pl
from jax.experimental.pallas import tpu as pltpu
from jax.sharding import PartitionSpec as P

HEAD_DIM = 64
PIECES = 4
GROUPS = 2


def route_weights(normed, group_router, expert_router, chosen, group_size):
    group_logits = jnp.dot(normed, group_router, preferred_element_type=jnp.float32)
    expert_logits = jnp.dot(normed, expert_router, preferred_element_type=jnp.float32)
    chosen_group = chosen[:, 0] // group_size
    margin = group_logits[:, 0] - group_logits[:, 1]
    own_margin = jnp.where(chosen_group == 0, margin, -margin)
    experts_iota = jnp.arange(expert_logits.shape[1], dtype=jnp.int32)
    picked = jnp.sum(
        jnp.where(
            chosen[:, :, None] == experts_iota[None, None, :],
            expert_logits[:, None, :],
            jnp.float32(0.0),
        ),
        axis=2,
    )
    return jax.nn.sigmoid(own_margin)[:, None] * jax.nn.sigmoid(picked - picked[:, ::-1])


def slot_table(chosen, expert_count, slots):
    flat_ids = chosen.reshape(-1)
    onehot = (flat_ids[:, None] == jnp.arange(expert_count, dtype=jnp.int32)[None, :]).astype(
        jnp.int32
    )
    before = jnp.cumsum(onehot, axis=0) - onehot
    ranks = jnp.sum(before * onehot, axis=1)
    return (flat_ids * slots + ranks).reshape(chosen.shape)


def dispatch(normed, slot_ids, total_slots):
    flat_slots = slot_ids.reshape(-1)
    owners = jnp.arange(flat_slots.shape[0], dtype=jnp.int32) // 2
    slot_iota = jnp.arange(total_slots, dtype=jnp.int32)
    token_of_slot = jnp.sum(
        jnp.where(slot_iota[:, None] == flat_slots[None, :], owners[None, :], 0), axis=1
    )
    return jnp.take(normed, token_of_slot, axis=0)


def expert_rows(row_block, gate_part, up_part, down_part):
    gate_val = jnp.dot(row_block, gate_part, preferred_element_type=jnp.float32)
    up_val = jnp.dot(row_block, up_part, preferred_element_type=jnp.float32)
    hidden = (jax.nn.silu(gate_val) * up_val).astype(jnp.bfloat16)
    return jnp.dot(hidden, down_part, preferred_element_type=jnp.float32).astype(jnp.bfloat16)


MESH_ID = pl.DeviceIdType.MESH
VMEM_SPEC = pl.BlockSpec(memory_space=pltpu.VMEM)
ANY_SPEC = pl.BlockSpec(memory_space=pl.ANY)
F32 = jnp.float32
BF16 = jnp.bfloat16


def remote(src, dst, send_sem, recv_sem, device):
    return pltpu.make_async_remote_copy(
        src_ref=src, dst_ref=dst, send_sem=send_sem, recv_sem=recv_sem,
        device_id=device, device_id_type=MESH_ID,
    )


def columns(piece, width):
    return pl.ds((piece % 2) * (width // 2), width // 2)


def greet(device):
    pl.semaphore_signal(
        pltpu.get_barrier_semaphore(), inc=1, device_id=device, device_id_type=MESH_ID
    )


class Line:
    def __init__(self, chips, chip, sp, tp, block, down_in, up_in, sems):
        self.chips, self.chip, self.me, self.block = chips, chip, (sp, tp), block
        down_send, down_recv, up_send, up_recv = sems
        self.legs = (
            (down_in, down_send, down_recv, (sp, tp - 2), chip < chips - 1),
            (up_in, up_send, up_recv, (sp, tp + 2), chip > 0),
        )

    def copy(self, leg, dest, p, device):
        inbox, send, recv = leg[:3]
        return remote(
            self.block(dest, p), inbox.at[dest, p], send.at[dest, p], recv.at[dest, p], device
        )

    def gather(self, leg, dest, p, device):
        @pl.when(leg[4])
        def _():
            self.copy(leg, dest, p, device).wait_recv()
            piece = self.block(dest, p)
            piece[...] = (piece[...].astype(F32) + leg[0][dest, p].astype(F32)).astype(BF16)

    def send(self, below, above, pieces, ready):
        chip, chips = self.chip, self.chips
        for p in pieces:
            for leg, dest, valid in (
                (self.legs[0], below, (below >= 0) & (below < chip)),
                (self.legs[1], above, (above > chip) & (above < chips)),
            ):

                @pl.when(valid)
                def _():
                    ready(dest, p)
                    self.gather(leg, dest, p, leg[3])
                    self.copy(leg, dest, p, leg[3]).start()

    def own(self, p, ready):
        ready(self.chip, p)
        for leg in self.legs:
            self.gather(leg, self.chip, p, leg[3])

    def drain(self):
        for dest in range(self.chips):
            for leg, sent in ((self.legs[0], dest < self.chip), (self.legs[1], dest > self.chip)):

                @pl.when(sent)
                def _():
                    for p in range(PIECES):
                        self.copy(leg, dest, p, leg[3]).wait_send()


def attention(
    sp_count, chips, heads, loads, later_loads,
    q_ref, k_ref, v_ref, off_ref, doc_ref,
    meta_ref, doc_col, k_buf, v_buf, m_buf, acc, carry, kv_send, kv_recv,
):
    sp = lax.axis_index("sp")
    tp = lax.axis_index("tp")
    chip = tp // 2
    core = tp % 2
    partner = tp + 1 - 2 * core
    tok, att = q_ref.shape
    for j in range(1, sp_count):
        greet((lax.rem(sp + j, sp_count), tp))
    greet((sp, partner))

    @pl.when(chip > 0)
    def _():
        greet((sp, tp - 2))

    @pl.when(chip < chips - 1)
    def _():
        greet((sp, tp + 2))

    expect = sp_count + jnp.where(chip > 0, 1, 0) + jnp.where(chip < chips - 1, 1, 0)
    docs = doc_ref[...].astype(F32)
    meta_ref[...] = jnp.zeros_like(meta_ref)
    meta_ref[0:heads, :] = off_ref[...].astype(F32)
    meta_ref[heads : heads + 1, :] = docs
    doc_col[...] = jnp.broadcast_to(docs, (128, tok)).T[:, :1]
    for copy in loads:
        copy.wait()
    pl.semaphore_wait(pltpu.get_barrier_semaphore(), expect)

    def kv_copies(j, target):
        return [
            remote(src, buf.at[j - 1], kv_send.at[j - 1, n], kv_recv.at[j - 1, n], (target, tp))
            for n, (src, buf) in enumerate(((k_ref, k_buf), (v_ref, v_buf), (meta_ref, m_buf)))
        ]

    for j in range(1, sp_count):

        @pl.when(sp + j < sp_count)
        def _():
            for copy in kv_copies(j, sp + j):
                copy.start()

    for copy in later_loads:
        copy.start()

    row = lax.broadcasted_iota(jnp.int32, (tok, tok), 0)
    col = lax.broadcasted_iota(jnp.int32, (tok, tok), 1)
    later = jnp.where(row > col, 1.0, 0.0).astype(BF16)
    lane = lax.broadcasted_iota(jnp.int32, (tok, att), 1) // HEAD_DIM
    acc[...] = jnp.zeros_like(acc)
    carry[...] = jnp.zeros_like(carry)

    def attend_block(keys, vals, meta, own):
        live = doc_col[...] == meta[heads : heads + 1, :]
        if own:
            live = live & (col < row)
        for h in range(heads):
            queries = jnp.where(lane == h, q_ref[...], jnp.zeros((), BF16)) * jnp.asarray(
                HEAD_DIM ** (-0.5), BF16
            )
            scores = lax.dot_general(
                queries, keys, (((1,), (1,)), ((), ())), preferred_element_type=F32
            ) + meta[h : h + 1, :]
            soft = jnp.maximum(scores, 0.0) + jnp.log(1.0 + jnp.exp(-jnp.abs(scores)))
            stay = jnp.where(live, -soft, 0.0)
            high = stay.astype(BF16)
            low = (stay - high.astype(F32)).astype(BF16)
            within = jnp.dot(high, later, preferred_element_type=F32) + jnp.dot(
                low, later, preferred_element_type=F32
            )
            before = carry[h]
            weights = jnp.where(
                live, jnp.exp(scores - soft + within + before), 0.0
            ).astype(BF16)
            out = jnp.dot(weights, vals, preferred_element_type=F32)
            acc[...] += jnp.where(lane == h, out, 0.0)
            carry[h] = before + within[:, :1] + stay[:, :1]

    attend_block(k_ref[...], v_ref[...], meta_ref[...], True)

    def earlier(j, unused):
        @pl.when(sp - j >= 0)
        def _():
            for copy in kv_copies(j, sp):
                copy.wait_recv()
            attend_block(k_buf[j - 1], v_buf[j - 1], m_buf[j - 1], False)

        return unused

    lax.fori_loop(1, sp_count, earlier, 0)

    def drain():
        for j in range(1, sp_count):

            @pl.when(sp + j < sp_count)
            def _():
                for copy in kv_copies(j, sp + j):
                    copy.wait_send()

    return acc[...].astype(BF16), drain


def project(attended, w_buf, part, chips, half_rows, first, last):
    tile = 512
    for n in range(first // tile, last // tile):
        cols = slice(n * tile, (n + 1) * tile)
        product = jnp.dot(attended, w_buf[:, cols], preferred_element_type=F32).astype(BF16)
        for z in range(chips):
            for c in range(2):
                for s in range(2):
                    at = ((z * 2 + c) * 2 + s) * half_rows
                    part[c, z, s, :, cols] = product[at : at + half_rows]


def mixer_kernel(
    sp_count, chips, heads,
    q_ref, k_ref, v_ref, off_ref, doc_ref, res_ref, gain_ref, w_hbm,
    mixed_ref, normed_ref,
    meta_ref, doc_col, k_buf, v_buf, m_buf, acc, carry, w_buf, part, partner_in, down_in, up_in,
    w_sem, kv_send, kv_recv, p_send, p_recv, down_send, down_recv, up_send, up_recv,
):
    sp = lax.axis_index("sp")
    tp = lax.axis_index("tp")
    chip = tp // 2
    core = tp % 2
    width = res_ref.shape[1]
    half_rows = res_ref.shape[0] // 2
    w_copy = pltpu.make_async_copy(w_hbm, w_buf, w_sem)
    attended, drain_kv = attention(
        sp_count, chips, heads, (), (w_copy,),
        q_ref, k_ref, v_ref, off_ref, doc_ref,
        meta_ref, doc_col, k_buf, v_buf, m_buf, acc, carry, kv_send, kv_recv,
    )
    w_copy.wait()
    project(attended, w_buf, part, chips, half_rows, 0, width)

    def p_copy(z):
        return remote(
            part.at[1 - core, z], partner_in.at[z], p_send.at[z, 0], p_recv.at[z, 0],
            (sp, tp + 1 - 2 * core),
        )

    for z in range(chips):
        p_copy(z).start()
    for z in range(chips):
        p_copy(z).wait_recv()
        part[core, z] = (part[core, z].astype(F32) + partner_in[z].astype(F32)).astype(BF16)
    line = Line(
        chips, chip, sp, tp, lambda z, p: part.at[core, z, p // 2, :, columns(p, width)],
        down_in, up_in, (down_send, down_recv, up_send, up_recv),
    )
    for distance in range(chips - 1, 0, -1):
        line.send(chip - distance, chip + distance, range(PIECES), lambda dest, p: None)
    for p in range(PIECES):
        line.own(p, lambda dest, p: None)
    total = part[core, chip].reshape(res_ref.shape).astype(F32)
    mixed = (res_ref[...].astype(F32) + total).astype(BF16)
    mixed_ref[...] = mixed
    mixed_f = mixed.astype(F32)
    scaling = lax.rsqrt(jnp.mean(mixed_f * mixed_f, axis=1, keepdims=True) + 1e-06)
    normed_ref[...] = (mixed_f * scaling * gain_ref[...]).astype(BF16)
    for z in range(chips):
        p_copy(z).wait_send()
    line.drain()
    drain_kv()


def mixer_scratch(residual, queries, heads, out_weight):
    sp_count = lax.axis_size("sp")
    chips = lax.axis_size("tp") // 2
    rows, width = residual.shape
    tok, att = queries.shape
    others = max(sp_count - 1, 1)
    half = (chips, 2, rows // 2, width)
    quarter = (chips, PIECES, rows // 2, width // 2)
    dma = pltpu.SemaphoreType.DMA
    meta_shape = (heads + 1 + -(heads + 1) % 8, tok)
    return [
        pltpu.VMEM(meta_shape, F32),
        pltpu.VMEM((tok, 1), F32),
        pltpu.VMEM((others, tok, att), BF16),
        pltpu.VMEM((others, tok, att), BF16),
        pltpu.VMEM((others,) + meta_shape, F32),
        pltpu.VMEM((tok, att), F32),
        pltpu.VMEM((heads, tok, 1), F32),
        pltpu.VMEM(out_weight.shape, BF16),
        pltpu.VMEM((2,) + half, BF16),
        pltpu.VMEM(half, BF16),
        pltpu.VMEM(quarter, BF16),
        pltpu.VMEM(quarter, BF16),
        dma,
        dma((others, 3)),
        dma((others, 3)),
        dma((chips, 2)),
        dma((chips, 2)),
    ] + [dma((chips, PIECES))] * 4


def mixer(residual, queries, keys, values, offsets, docs, out_weight, gain):
    heads = offsets.shape[1]
    return pl.pallas_call(
        functools.partial(
            mixer_kernel, lax.axis_size("sp"), lax.axis_size("tp") // 2, heads
        ),
        out_shape=[jax.ShapeDtypeStruct(residual.shape, BF16)] * 2,
        in_specs=[VMEM_SPEC] * 7 + [ANY_SPEC],
        out_specs=[VMEM_SPEC] * 2,
        scratch_shapes=mixer_scratch(residual, queries, heads, out_weight),
        compiler_params=pltpu.CompilerParams(
            collective_id=0, has_side_effects=True, vmem_limit_bytes=48 << 20
        ),
        name="mixer",
    )(queries, keys, values, offsets.T, docs[None, :], residual, gain[None, :], out_weight)


def slot_row(ids, tp, rows):
    tok = ids.shape[1]
    group = jnp.broadcast_to((ids[:1, :] // 2).astype(F32), (8, tok)).astype(BF16)
    at = lax.broadcasted_iota(jnp.int32, (tok, 128), 0)
    lane = lax.broadcasted_iota(jnp.int32, (tok, 128), 1)
    pick = jnp.where(at == lane + tp * rows, 1.0, 0.0).astype(BF16)
    mine = jnp.dot(group, pick, preferred_element_type=F32)
    before_at = lax.broadcasted_iota(jnp.int32, (128, 128), 0)
    before_lane = lax.broadcasted_iota(jnp.int32, (128, 128), 1)
    before = jnp.where(before_at < before_lane, 1.0, 0.0).astype(BF16)
    ones = jnp.dot(mine.astype(BF16), before, preferred_element_type=F32)
    token = lax.broadcasted_iota(jnp.int32, (8, 128), 1).astype(F32)
    slot = jnp.where(mine > 0.5, ones + rows // 2, token - ones)
    return slot[:1, :rows]


def experts_kernel(
    chips,
    w_copies, w_copy, res_copy, attended,
    mixed_ref, res_ref, gain_ref, ids_ref, group_ref, expert_ref,
    out_ref,
    w_buf, sums, sums_in, a_down_in, a_up_in, a_send, a_recv, a_sems,
    router_ref, gate, up, down, rows, y_out, part, partner_in, x_in, down_in, up_in, y_in, total,
    y_sem, rows_recv, line_send, x_send, fan_send,
    p_send, p_recv, xr_send, xr_recv, down_send, down_recv, up_send, up_recv,
):
    sp = lax.axis_index("sp")
    tp = lax.axis_index("tp")
    y, x = sp // 2, sp % 2
    chip, core = tp // 2, tp % 2
    partner = (sp, tp + 1 - 2 * core)
    x_peer = (sp + 1 - 2 * x, tp)
    y_peer = (lax.rem(sp + 2, 4), tp)
    below, above = (sp, tp - 2), (sp, tp + 2)
    has_below, has_above = chip > 0, chip < chips - 1
    row_count, width = res_ref.shape
    half_rows = row_count // 2
    half_width = width // 2

    slots = slot_row(ids_ref[...], tp, row_count)
    slot_iota = lax.broadcasted_iota(jnp.int32, (half_rows, row_count), 0)

    def selection(group):
        wanted = (slot_iota + group * half_rows).astype(F32)
        return jnp.where(wanted == slots, 1.0, 0.0).astype(BF16)

    sel_own, sel_other = selection(y), selection(1 - y)
    router_ref[...] = jnp.zeros_like(router_ref)
    router_ref[0:2, :] = group_ref[...].astype(F32)
    router_ref[2:6, :] = expert_ref[...].astype(F32)

    def span(h):
        return columns(h, width)

    def y_copy(h):
        return remote(
            y_out.at[:, span(h)], rows.at[x, chip, core, y, :, span(h)], y_sem.at[5 + h],
            rows_recv.at[x, chip, core, y, h], y_peer,
        )

    def piece_copy(xs, z, c, s, h, send, device):
        piece = rows.at[xs, z, c, s, :, span(h)]
        return remote(piece, piece, send, rows_recv.at[xs, z, c, s, h], device)

    def line_piece(z, s, h, up_ok, down_ok, act):
        @pl.when(down_ok)
        def _():
            act(piece_copy(x, z, core, s, h, line_send.at[z, s, 0, h], below))

        @pl.when(up_ok)
        def _():
            act(piece_copy(x, z, core, s, h, line_send.at[z, s, 1, h], above))

        act(piece_copy(x, z, core, s, h, x_send.at[z, s, h], x_peer))
        act(piece_copy(x, z, core, s, h, fan_send.at[0, z, s, h], partner))

    def begin(copy):
        copy.start()

    def arrived(xs, z, c, s, h):
        piece_copy(xs, z, c, s, h, y_sem.at[0], x_peer).wait_recv()

    def own_rest(s):
        for h in range(2):
            arrived(x, chip, core, s, h)
            line_piece(chip, s, h, has_above, has_below, begin)

    def line_pieces(distance, s, act, wait):
        for h in range(2):

            @pl.when(chip - distance >= 0)
            def _():
                if wait:
                    arrived(x, chip - distance, core, s, h)
                line_piece(chip - distance, s, h, has_above, chip < 0, act)

            @pl.when(chip + distance < chips)
            def _():
                if wait:
                    arrived(x, chip + distance, core, s, h)
                line_piece(chip + distance, s, h, chip < 0, has_below, act)

    def at_distance(distance, body):
        if distance == 0:
            body(chip)
            return

        @pl.when(chip - distance >= 0)
        def _():
            body(chip - distance)

        @pl.when(chip + distance < chips)
        def _():
            body(chip + distance)

    def cross(z, s, act, wait):
        for h in range(2):
            if wait:
                arrived(1 - x, z, core, s, h)
            act(piece_copy(1 - x, z, core, s, h, fan_send.at[1, z, s, h], partner))

    def a_copy(z, h):
        cols = columns(h, width)
        return remote(
            sums.at[1 - core, z, :, :, cols], sums_in.at[z, :, :, cols], a_send.at[z, h],
            a_recv.at[z, h], partner,
        )

    w_copy.wait()
    for h in range(2):
        project(attended, w_buf, sums, chips, half_rows, h * half_width, (h + 1) * half_width)
        for z in range(chips):
            a_copy(z, h).start()

    def fold(dest, p):
        if p < 2:
            cols = columns(p, width)
            a_copy(dest, p).wait_recv()
            sums[core, dest, :, :, cols] = (
                sums[core, dest, :, :, cols].astype(F32) + sums_in[dest, :, :, cols].astype(F32)
            ).astype(BF16)

    mix = Line(
        chips, chip, sp, tp, lambda z, p: sums.at[core, z, p // 2, :, columns(p, width)],
        a_down_in, a_up_in, a_sems,
    )

    def settle():
        for p in range(PIECES):
            mix.own(p, fold)
        added = sums[core, chip].reshape(row_count, width).astype(F32)
        mixed = (res_ref[...].astype(F32) + added).astype(BF16)
        mixed_ref[...] = mixed
        mixed_f = mixed.astype(F32)
        scaling = lax.rsqrt(jnp.mean(mixed_f * mixed_f, axis=1, keepdims=True) + 1e-06)
        normed = (mixed_f * scaling * gain_ref[...]).astype(BF16)
        for h in range(2):
            cols = slice(h * half_width, (h + 1) * half_width)
            y_out[:, cols] = jnp.dot(
                sel_other, normed[:, cols], preferred_element_type=F32
            ).astype(BF16)
            y_copy(h).start()
            rows[x, chip, core, y, :, cols] = jnp.dot(
                sel_own, normed[:, cols], preferred_element_type=F32
            ).astype(BF16)
            line_piece(chip, y, h, has_above, has_below, begin)

    def p_copy(z):
        return remote(part.at[z, 1 - core], partner_in.at[z], p_send.at[z], p_recv.at[z], partner)

    def xr_copy(z, s):
        return remote(
            part.at[z, core, 1 - x, s], x_in.at[z, s], xr_send.at[z, s], xr_recv.at[z, s], x_peer
        )

    lanes = lax.broadcasted_iota(jnp.int32, (1, router_ref.shape[0]), 1)

    def signed(plus, minus):
        return jnp.where(lanes == plus, 1.0, 0.0) - jnp.where(lanes == minus, 1.0, 0.0)

    group_sign = signed(y, 1 - y)
    expert_sign = signed(2 + sp, 2 + sp + 1 - 2 * x)

    def expert(z):
        for h in range(2):
            for xs in range(2):
                for s in range(2):
                    arrived(xs, z, 1 - core, s, h)
        block = rows[:, z].reshape(8 * half_rows, width)
        logits = lax.dot_general(
            block, router_ref[...].astype(BF16), (((1,), (1,)), ((), ())), preferred_element_type=F32
        )
        route = jax.nn.sigmoid(
            jnp.sum(logits * group_sign, axis=1, keepdims=True)
        ) * jax.nn.sigmoid(jnp.sum(logits * expert_sign, axis=1, keepdims=True))
        gated = jnp.dot(block, gate[...], preferred_element_type=F32)
        raised = jnp.dot(block, up[...], preferred_element_type=F32)
        hidden = (jax.nn.silu(gated) * raised).astype(BF16)
        tile = 1024
        for n in range(width // tile):
            cols = slice(n * tile, (n + 1) * tile)
            out = jnp.dot(hidden, down[:, cols], preferred_element_type=F32) * route
            out = out.astype(BF16)
            for xs in range(2):
                for c in range(2):
                    for s in range(2):
                        at = ((xs * 2 + c) * 2 + s) * half_rows
                        part[z, c, xs, s, :, cols] = out[at : at + half_rows]
        p_copy(z).start()

    halves = (1 - y, y)

    def send_x(z, s):
        xr_copy(z, s).start()

    def join_cores(z, send=True):
        p_copy(z).wait_recv()
        for xs in (1 - x, x):
            for s in halves:
                part[z, core, xs, s] = (
                    part[z, core, xs, s].astype(F32) + partner_in[z, xs, s].astype(F32)
                ).astype(BF16)
                if xs is not x and send:
                    xr_copy(z, s).start()

    def join_x(z, piece):
        s = halves[piece // 2]
        if piece % 2 == 0:
            xr_copy(z, s).wait_recv()
            part[z, core, x, s] = (
                part[z, core, x, s].astype(F32) + x_in[z, s].astype(F32)
            ).astype(BF16)

    def back_copy(n):
        cols = columns(n, width)
        return remote(
            part.at[chip, core, x, 1 - y, :, cols], y_in.at[:, cols], y_sem.at[1 + n],
            y_sem.at[3 + n], y_peer,
        )

    def finished(piece):
        cols = columns(piece, width)
        if piece < 2:
            back_copy(piece).start()
        else:
            sums = lax.dot_general(
                sel_own, part[chip, core, x, y, :, cols], (((0,), (0,)), ((), ())),
                preferred_element_type=F32,
            )
            total[:, cols] = mixed_ref[:, cols].astype(F32) + sums

    for distance in range(chips - 1, 0, -1):
        mix.send(chip - distance, chip + distance, range(PIECES), fold)
    res_copy.wait()

    def cross_all(distance, s):
        at_distance(distance, lambda z: cross(z, s, begin, True))

    @pl.when(y == 0)
    def _():
        settle()

    @pl.when(y == 1)
    def _():
        own_rest(0)
        settle()

    line_pieces(1, 0, begin, True)

    @pl.when(y == 1)
    def _():
        line_pieces(1, 1, begin, True)

    line_pieces(2, 0, begin, True)

    @pl.when(y == 0)
    def _():
        own_rest(1)
        line_pieces(1, 1, begin, True)

    cross_all(0, 0)
    cross_all(1, 0)
    cross_all(0, 1)
    for copy in w_copies:
        copy.wait()
    is_end = (chip == 0) | (chip == chips - 1)

    at_distance(0, expert)
    line_pieces(2, 1, begin, True)
    cross_all(1, 1)
    at_distance(1, expert)
    at_distance(0, lambda z: join_cores(z, False))
    for s in range(2):
        line_pieces(3, s, begin, True)
        cross_all(2, s)
    at_distance(1, join_cores)
    at_distance(2, expert)

    @pl.when(is_end)
    def _():
        send_x(chip, 1 - y)

    for s in range(2):
        cross_all(3, s)
    at_distance(2, lambda z: join_cores(z, False))

    @pl.when(jnp.logical_not(is_end))
    def _():
        for s in halves:
            at_distance(2, lambda z: send_x(z, s))
        send_x(chip, 1 - y)

    at_distance(3, expert)
    at_distance(3, join_cores)

    @pl.when(is_end)
    def _():
        for s in halves:
            at_distance(2, lambda z: send_x(z, s))

    send_x(chip, y)
    back = Line(
        chips, chip, sp, tp,
        lambda z, p: part.at[z, core, x, halves[p // 2], :, columns(p, width)],
        down_in, up_in, (down_send, down_recv, up_send, up_recv),
    )
    def back_turn(distance, mine):
        back.send(
            jnp.where(mine, chip - distance, -1), jnp.where(mine, chip + distance, chips),
            range(PIECES), join_x,
        )

    back_turn(1, is_end)
    for distance in range(chips - 1, 1, -1):
        back_turn(distance, True)
    back_turn(1, jnp.logical_not(is_end))
    for p in range(PIECES):
        back.own(p, join_x)
        finished(p)
    for n in range(2):
        cols = columns(n, width)
        back_copy(n).wait_recv()
        returned = lax.dot_general(
            sel_other, y_in[:, cols], (((0,), (0,)), ((), ())), preferred_element_type=F32
        )
        out_ref[:, cols] = (total[:, cols] + returned).astype(BF16)

    def end(copy):
        copy.wait_send()

    for n in range(2):
        back_copy(n).wait_send()
    for h in range(2):
        y_copy(h).wait_send()
        for s in range(2):
            line_piece(chip, s, h, has_above, has_below, end)
        for z in range(chips):
            end(a_copy(z, h))
    for s in range(2):
        for distance in range(chips):
            if distance:
                line_pieces(distance, s, end, False)
            at_distance(distance, lambda z: cross(z, s, end, False))
    for z in range(chips):
        end(p_copy(z))
        for s in range(2):
            end(xr_copy(z, s))
    mix.drain()
    back.drain()


def layer_kernel(
    sp_count, chips, heads, mixer_count,
    q_hbm, k_hbm, v_hbm, res_hbm, w_hbm, gate_hbm, up_hbm, down_hbm,
    off_ref, doc_ref, gain_ref, ids_ref, group_ref, expert_ref,
    out_ref,
    q_ref, k_ref, v_ref, res_ref, mixed_ref, load_sem, weight_sem, router_ref,
    gate, up, down,
    *scratch,
):
    loads = [
        pltpu.make_async_copy(src, dst, load_sem.at[n])
        for n, (src, dst) in enumerate(
            ((k_hbm, k_ref), (v_hbm, v_ref), (q_hbm, q_ref), (res_hbm, res_ref))
        )
    ]
    weights = [
        pltpu.make_async_copy(src.at[0], dst, weight_sem.at[n])
        for n, (src, dst) in enumerate(((gate_hbm, gate), (up_hbm, up), (down_hbm, down)))
    ]
    for copy in loads[:3]:
        copy.start()
    (
        meta_ref, doc_col, k_buf, v_buf, m_buf, acc, carry, w_buf, sums, sums_in, a_down_in, a_up_in,
        w_sem, kv_send, kv_recv, a_send, a_recv,
    ) = scratch[: mixer_count - 4]
    a_sems = scratch[mixer_count - 4 : mixer_count]
    w_copy = pltpu.make_async_copy(w_hbm, w_buf, w_sem)
    attended, drain_kv = attention(
        sp_count, chips, heads, loads[:3], [w_copy, loads[3]] + weights,
        q_ref, k_ref, v_ref, off_ref, doc_ref,
        meta_ref, doc_col, k_buf, v_buf, m_buf, acc, carry, kv_send, kv_recv,
    )
    experts_kernel(
        chips, weights, w_copy, loads[3], attended,
        mixed_ref, res_ref, gain_ref, ids_ref, group_ref, expert_ref, out_ref,
        w_buf, sums, sums_in, a_down_in, a_up_in, a_send, a_recv, a_sems,
        router_ref, gate, up, down, *scratch[mixer_count:],
    )
    drain_kv()


def pair_layer(
    residual, queries, keys, values, offsets, docs, out_weight, gain,
    expert_ids, group_router, expert_router, gate, up, down,
):
    chips = lax.axis_size("tp") // 2
    rows, width = residual.shape
    heads = offsets.shape[1]
    mixer_parts = mixer_scratch(residual, queries, heads, out_weight)
    half_rows = rows // 2
    units = gate.shape[2]
    half = (chips, 2, half_rows, width)
    quarter = (chips, PIECES, half_rows, width // 2)
    dma = pltpu.SemaphoreType.DMA
    return pl.pallas_call(
        functools.partial(
            layer_kernel, lax.axis_size("sp"), chips, heads, len(mixer_parts)
        ),
        out_shape=jax.ShapeDtypeStruct((rows, width), BF16),
        in_specs=[ANY_SPEC] * 8 + [VMEM_SPEC] * 6,
        out_specs=VMEM_SPEC,
        scratch_shapes=[
            pltpu.VMEM(queries.shape, BF16),
            pltpu.VMEM(keys.shape, BF16),
            pltpu.VMEM(values.shape, BF16),
            pltpu.VMEM((rows, width), BF16),
            pltpu.VMEM((rows, width), BF16),
            dma((4,)),
            dma((3,)),
            pltpu.VMEM((8, width), F32),
            pltpu.VMEM((width, units), BF16),
            pltpu.VMEM((width, units), BF16),
            pltpu.VMEM((units, width), BF16),
        ]
        + mixer_parts
        + [
            pltpu.VMEM((2, chips, 2, 2, half_rows, width), BF16),
            pltpu.VMEM((half_rows, width), BF16),
            pltpu.VMEM((chips, 2, 2, 2, half_rows, width), BF16),
            pltpu.VMEM((chips, 2, 2, half_rows, width), BF16),
            pltpu.VMEM(half, BF16),
            pltpu.VMEM(quarter, BF16),
            pltpu.VMEM(quarter, BF16),
            pltpu.VMEM((half_rows, width), BF16),
            pltpu.VMEM((rows, width), F32),
            dma((7,)),
            dma((2, chips, 2, 2, 2)),
            dma((chips, 2, 2, 2)),
            dma((chips, 2, 2)),
            dma((2, chips, 2, 2)),
            dma((chips,)),
            dma((chips,)),
            dma((chips, 2)),
            dma((chips, 2)),
        ]
        + [dma((chips, PIECES))] * 4,
        compiler_params=pltpu.CompilerParams(
            collective_id=1, has_side_effects=True, vmem_limit_bytes=60 << 20
        ),
        name="layer",
    )(
        queries, keys, values, residual, out_weight, gate, up, down,
        offsets.T, docs[None, :], gain[None, :], expert_ids.T, group_router.T, expert_router.T,
    )


def per_device(
    residual_in,
    queries,
    keys,
    values,
    break_offset,
    doc_ids,
    out_weight,
    norm_gain,
    group_router,
    expert_router,
    expert_ids,
    gate_weight,
    up_weight,
    down_weight,
):
    tok_dev = queries.shape[0]
    sp_count = lax.axis_size("sp")
    tp_count = lax.axis_size("tp")
    tp_rank = lax.axis_index("tp")
    width = residual_in.shape[1]
    rows_dev = tok_dev // tp_count
    chosen = lax.dynamic_slice_in_dim(expert_ids, tp_rank * rows_dev, rows_dev, 0)
    expert_count = sp_count * gate_weight.shape[0]
    group_size = expert_count // GROUPS
    if sp_count == 4 and gate_weight.shape[0] == 1 and rows_dev % 32 == 0:
        return pair_layer(
            residual_in, queries, keys, values, break_offset, doc_ids, out_weight, norm_gain,
            expert_ids, group_router, expert_router, gate_weight, up_weight, down_weight,
        )
    mixed_stream, normed = mixer(
        residual_in, queries, keys, values, break_offset, doc_ids, out_weight, norm_gain
    )
    routes = route_weights(normed, group_router, expert_router, chosen, group_size)
    slots = 2 * rows_dev // expert_count
    slot_ids = slot_table(chosen, expert_count, slots)
    sent = dispatch(normed, slot_ids, expert_count * slots).reshape(expert_count, slots, width)
    fanned = lax.all_gather(
        lax.all_to_all(sent, "sp", split_axis=0, concat_axis=0, tiled=True),
        "tp",
        axis=0,
        tiled=True,
    )
    partial_out = expert_rows(
        fanned.reshape(-1, width), gate_weight[0], up_weight[0], down_weight[0]
    )
    unit_total = lax.psum_scatter(
        partial_out.reshape(fanned.shape), "tp", scatter_dimension=0, tiled=True
    ).astype(jnp.float32)
    returned = lax.all_to_all(
        unit_total.astype(jnp.bfloat16), "sp", split_axis=0, concat_axis=0, tiled=True
    )
    expert_out = jnp.take(returned.reshape(-1, width), slot_ids.reshape(-1), axis=0).reshape(
        rows_dev, 2, width
    )
    mixture = jnp.sum(routes[:, :, None] * expert_out.astype(jnp.float32), axis=1)
    return (mixed_stream.astype(jnp.float32) + mixture).astype(jnp.bfloat16)


def solution(mesh):
    return jax.shard_map(
        per_device,
        mesh=mesh,
        in_specs=(
            P(("sp", "tp"), None),
            P("sp", "tp"),
            P("sp", "tp"),
            P("sp", "tp"),
            P("sp", "tp"),
            P("sp"),
            P("tp", None),
            P(),
            P(),
            P(),
            P("sp", None),
            P("sp", None, "tp"),
            P("sp", None, "tp"),
            P("sp", "tp", None),
        ),
        out_specs=P(("sp", "tp"), None),
        check_vma=False,
    )
```

```python
import functools

import jax
import jax.numpy as jnp
from jax import lax
from jax.experimental import pallas as pl
from jax.experimental.pallas import tpu as pltpu
from jax.sharding import PartitionSpec as P

HEAD_DIM = 64
PIECES = 4
GROUPS = 2


def route_weights(normed, group_router, expert_router, chosen, group_size):
    group_logits = jnp.dot(normed, group_router, preferred_element_type=jnp.float32)
    expert_logits = jnp.dot(normed, expert_router, preferred_element_type=jnp.float32)
    chosen_group = chosen[:, 0] // group_size
    margin = group_logits[:, 0] - group_logits[:, 1]
    own_margin = jnp.where(chosen_group == 0, margin, -margin)
    experts_iota = jnp.arange(expert_logits.shape[1], dtype=jnp.int32)
    picked = jnp.sum(
        jnp.where(
            chosen[:, :, None] == experts_iota[None, None, :],
            expert_logits[:, None, :],
            jnp.float32(0.0),
        ),
        axis=2,
    )
    return jax.nn.sigmoid(own_margin)[:, None] * jax.nn.sigmoid(picked - picked[:, ::-1])


def slot_table(chosen, expert_count, slots):
    flat_ids = chosen.reshape(-1)
    onehot = (flat_ids[:, None] == jnp.arange(expert_count, dtype=jnp.int32)[None, :]).astype(
        jnp.int32
    )
    before = jnp.cumsum(onehot, axis=0) - onehot
    ranks = jnp.sum(before * onehot, axis=1)
    return (flat_ids * slots + ranks).reshape(chosen.shape)


def dispatch(normed, slot_ids, total_slots):
    flat_slots = slot_ids.reshape(-1)
    owners = jnp.arange(flat_slots.shape[0], dtype=jnp.int32) // 2
    slot_iota = jnp.arange(total_slots, dtype=jnp.int32)
    token_of_slot = jnp.sum(
        jnp.where(slot_iota[:, None] == flat_slots[None, :], owners[None, :], 0), axis=1
    )
    return jnp.take(normed, token_of_slot, axis=0)


def expert_rows(row_block, gate_part, up_part, down_part):
    gate_val = jnp.dot(row_block, gate_part, preferred_element_type=jnp.float32)
    up_val = jnp.dot(row_block, up_part, preferred_element_type=jnp.float32)
    hidden = (jax.nn.silu(gate_val) * up_val).astype(jnp.bfloat16)
    return jnp.dot(hidden, down_part, preferred_element_type=jnp.float32).astype(jnp.bfloat16)


MESH_ID = pl.DeviceIdType.MESH
VMEM_SPEC = pl.BlockSpec(memory_space=pltpu.VMEM)
ANY_SPEC = pl.BlockSpec(memory_space=pl.ANY)
F32 = jnp.float32
BF16 = jnp.bfloat16


def remote(src, dst, send_sem, recv_sem, device):
    return pltpu.make_async_remote_copy(
        src_ref=src, dst_ref=dst, send_sem=send_sem, recv_sem=recv_sem,
        device_id=device, device_id_type=MESH_ID,
    )


def columns(piece, width):
    return pl.ds((piece % 2) * (width // 2), width // 2)


def greet(device):
    pl.semaphore_signal(
        pltpu.get_barrier_semaphore(), inc=1, device_id=device, device_id_type=MESH_ID
    )


class Line:
    def __init__(self, chips, chip, sp, tp, whole, block, down_in, up_in, sems):
        self.chips, self.chip, self.whole, self.block = chips, chip, whole, block
        down_send, down_recv, up_send, up_recv = sems
        self.legs = (
            (down_in, down_send, down_recv, (sp, tp - 2), chip < chips - 1),
            (up_in, up_send, up_recv, (sp, tp + 2), chip > 0),
        )

    def copy(self, leg, dest, p, device):
        inbox, send, recv = leg[:3]
        return remote(
            self.block(dest, p), inbox.at[dest, p], send.at[dest], recv.at[dest, p], device
        )

    def gather(self, leg, dest, p, device):
        @pl.when(leg[4])
        def _():
            self.copy(leg, dest, p, device).wait_recv()
            piece = self.block(dest, p)
            piece[...] = (piece[...].astype(F32) + leg[0][dest, p].astype(F32)).astype(BF16)

    def send(self, below, above, pieces, ready):
        chip, chips = self.chip, self.chips
        for p in pieces:
            for leg, dest, valid in (
                (self.legs[0], below, (below >= 0) & (below < chip)),
                (self.legs[1], above, (above > chip) & (above < chips)),
            ):

                @pl.when(valid)
                def _():
                    ready(dest, p)
                    self.gather(leg, dest, p, leg[3])
                    self.copy(leg, dest, p, leg[3]).start()

    def own(self, p, ready):
        ready(self.chip, p)
        for leg in self.legs:
            self.gather(leg, self.chip, p, leg[3])

    def drain(self):
        for dest in range(self.chips):
            for leg, sent in ((self.legs[0], dest < self.chip), (self.legs[1], dest > self.chip)):

                @pl.when(sent)
                def _():
                    chunk = self.whole(dest)
                    remote(
                        chunk, chunk, leg[1].at[dest], leg[2].at[dest, 0], leg[3]
                    ).wait_send()


def attention(
    sp_count, chips, heads, relay, loads, later_loads,
    q_ref, k_ref, v_ref, off_ref, doc_ref,
    meta_ref, doc_col, k_buf, v_buf, m_buf, acc, carry, kv_send, kv_recv,
):
    sp = lax.axis_index("sp")
    tp = lax.axis_index("tp")
    chip = tp // 2
    core = tp % 2
    partner = tp + 1 - 2 * core
    tok, att = q_ref.shape
    for j in range(1, sp_count):
        greet((lax.rem(sp + j, sp_count), tp))
    greet((sp, partner))

    @pl.when(chip > 0)
    def _():
        greet((sp, tp - 2))

    @pl.when(chip < chips - 1)
    def _():
        greet((sp, tp + 2))

    expect = sp_count + jnp.where(chip > 0, 1, 0) + jnp.where(chip < chips - 1, 1, 0)
    docs = doc_ref[...].astype(F32)
    meta_ref[...] = jnp.zeros_like(meta_ref)
    meta_ref[0:heads, :] = off_ref[...].astype(F32)
    meta_ref[heads : heads + 1, :] = docs
    doc_col[...] = jnp.broadcast_to(docs, (128, tok)).T[:, :1]
    for copy in loads:
        copy.wait()
    pl.semaphore_wait(pltpu.get_barrier_semaphore(), expect)

    def kv_copies(j, target):
        return [
            remote(src, buf.at[j - 1], kv_send.at[j - 1, n], kv_recv.at[j - 1, n], (target, tp))
            for n, (src, buf) in enumerate(((k_ref, k_buf), (v_ref, v_buf), (meta_ref, m_buf)))
        ]

    def sends(act):
        for j in range(1, sp_count):
            keys, *others = kv_copies(j, sp + j)
            direct = sp + j < sp_count

            @pl.when(direct & (sp + j != sp_count - 1 - sp) if relay else direct)
            def _():
                act(keys)

            @pl.when(direct)
            def _():
                for copy in others:
                    act(copy)

    def relayed():
        slot = 2 * x_peer - sp_count
        return remote(
            k_buf.at[1], k_buf.at[slot], kv_send.at[2, 0], kv_recv.at[slot, 0], (x_peer, tp)
        )

    x_peer = sp + 1 - 2 * (sp % 2)
    sends(lambda copy: copy.start())

    for copy in later_loads:
        copy.start()

    row = lax.broadcasted_iota(jnp.int32, (tok, tok), 0)
    col = lax.broadcasted_iota(jnp.int32, (tok, tok), 1)
    later = jnp.where(row > col, 1.0, 0.0).astype(BF16)
    lane = lax.broadcasted_iota(jnp.int32, (tok, att), 1) // HEAD_DIM
    acc[...] = jnp.zeros_like(acc)
    carry[...] = jnp.zeros_like(carry)

    def attend_block(keys, vals, meta, own):
        live = doc_col[...] == meta[heads : heads + 1, :]
        if own:
            live = live & (col < row)
        for h in range(heads):
            queries = jnp.where(lane == h, q_ref[...], jnp.zeros((), BF16)) * jnp.asarray(
                HEAD_DIM ** (-0.5), BF16
            )
            scores = lax.dot_general(
                queries, keys, (((1,), (1,)), ((), ())), preferred_element_type=F32
            ) + meta[h : h + 1, :]
            soft = jnp.maximum(scores, 0.0) + jnp.log(1.0 + jnp.exp(-jnp.abs(scores)))
            stay = jnp.where(live, -soft, 0.0)
            high = stay.astype(BF16)
            low = (stay - high.astype(F32)).astype(BF16)
            within = jnp.dot(high, later, preferred_element_type=F32) + jnp.dot(
                low, later, preferred_element_type=F32
            )
            before = carry[h]
            weights = jnp.where(
                live, jnp.exp(scores - soft + within + before), 0.0
            ).astype(BF16)
            out = jnp.dot(weights, vals, preferred_element_type=F32)
            acc[...] += jnp.where(lane == h, out, 0.0)
            carry[h] = before + within[:, :1] + stay[:, :1]

    attend_block(k_ref[...], v_ref[...], meta_ref[...], True)

    if relay:

        @pl.when(sp >= 2)
        def _():
            kv_copies(2, sp)[0].wait_recv()
            relayed().start()

    def earlier(j, unused):
        @pl.when(sp - j >= 0)
        def _():
            keys, *others = kv_copies(j, sp)

            @pl.when((sp < 2) | (j != 2) if relay else True)
            def _():
                keys.wait_recv()

            for copy in others:
                copy.wait_recv()
            attend_block(k_buf[j - 1], v_buf[j - 1], m_buf[j - 1], False)

        return unused

    lax.fori_loop(1, sp_count, earlier, 0)

    def drain():
        sends(lambda copy: copy.wait_send())
        if relay:

            @pl.when(sp >= 2)
            def _():
                relayed().wait_send()

    return acc[...].astype(BF16), drain


def project(attended, w_buf, part, chips, half_rows, first, last):
    tile = 512
    for n in range(first // tile, last // tile):
        cols = slice(n * tile, (n + 1) * tile)
        product = jnp.dot(attended, w_buf[:, cols], preferred_element_type=F32).astype(BF16)
        for z in range(chips):
            for c in range(2):
                for s in range(2):
                    at = ((z * 2 + c) * 2 + s) * half_rows
                    part[c, z, s, :, cols] = product[at : at + half_rows]


def mixer_kernel(
    sp_count, chips, heads,
    q_ref, k_ref, v_ref, off_ref, doc_ref, res_ref, gain_ref, w_hbm,
    mixed_ref, normed_ref,
    meta_ref, doc_col, k_buf, v_buf, m_buf, acc, carry, w_buf, part, partner_in, down_in, up_in,
    w_sem, kv_send, kv_recv, p_send, p_recv, down_send, down_recv, up_send, up_recv,
):
    sp = lax.axis_index("sp")
    tp = lax.axis_index("tp")
    chip = tp // 2
    core = tp % 2
    width = res_ref.shape[1]
    half_rows = res_ref.shape[0] // 2
    w_copy = pltpu.make_async_copy(w_hbm, w_buf, w_sem)
    attended, drain_kv = attention(
        sp_count, chips, heads, False, (), (w_copy,),
        q_ref, k_ref, v_ref, off_ref, doc_ref,
        meta_ref, doc_col, k_buf, v_buf, m_buf, acc, carry, kv_send, kv_recv,
    )
    w_copy.wait()
    project(attended, w_buf, part, chips, half_rows, 0, width)

    def p_copy(z):
        return remote(
            part.at[1 - core, z], partner_in.at[z], p_send.at[z], p_recv.at[z, 0],
            (sp, tp + 1 - 2 * core),
        )

    for z in range(chips):
        p_copy(z).start()
    for z in range(chips):
        p_copy(z).wait_recv()
        part[core, z] = (part[core, z].astype(F32) + partner_in[z].astype(F32)).astype(BF16)
    line = Line(
        chips, chip, sp, tp, lambda z: part.at[core, z],
        lambda z, p: part.at[core, z, p // 2, :, columns(p, width)],
        down_in, up_in, (down_send, down_recv, up_send, up_recv),
    )
    for distance in range(chips - 1, 0, -1):
        line.send(chip - distance, chip + distance, range(PIECES), lambda dest, p: None)
    for p in range(PIECES):
        line.own(p, lambda dest, p: None)
    total = part[core, chip].reshape(res_ref.shape).astype(F32)
    mixed = (res_ref[...].astype(F32) + total).astype(BF16)
    mixed_ref[...] = mixed
    mixed_f = mixed.astype(F32)
    scaling = lax.rsqrt(jnp.mean(mixed_f * mixed_f, axis=1, keepdims=True) + 1e-06)
    normed_ref[...] = (mixed_f * scaling * gain_ref[...]).astype(BF16)
    for z in range(chips):
        p_copy(z).wait_send()
    line.drain()
    drain_kv()


def mixer_scratch(residual, queries, heads, out_weight):
    sp_count = lax.axis_size("sp")
    chips = lax.axis_size("tp") // 2
    rows, width = residual.shape
    tok, att = queries.shape
    others = max(sp_count - 1, 1)
    half = (chips, 2, rows // 2, width)
    quarter = (chips, PIECES, rows // 2, width // 2)
    dma = pltpu.SemaphoreType.DMA
    meta_shape = (heads + 1 + -(heads + 1) % 8, tok)
    return [
        pltpu.VMEM(meta_shape, F32),
        pltpu.VMEM((tok, 1), F32),
        pltpu.VMEM((others, tok, att), BF16),
        pltpu.VMEM((others, tok, att), BF16),
        pltpu.VMEM((others,) + meta_shape, F32),
        pltpu.VMEM((tok, att), F32),
        pltpu.VMEM((heads, tok, 1), F32),
        pltpu.VMEM(out_weight.shape, BF16),
        pltpu.VMEM((2,) + half, BF16),
        pltpu.VMEM(half, BF16),
        pltpu.VMEM(quarter, BF16),
        pltpu.VMEM(quarter, BF16),
        dma,
        dma((others, 3)),
        dma((others, 3)),
        dma((chips,)),
        dma((chips, 2)),
    ] + [dma((chips,)), dma((chips, PIECES))] * 2


def mixer(residual, queries, keys, values, offsets, docs, out_weight, gain):
    heads = offsets.shape[1]
    return pl.pallas_call(
        functools.partial(
            mixer_kernel, lax.axis_size("sp"), lax.axis_size("tp") // 2, heads
        ),
        out_shape=[jax.ShapeDtypeStruct(residual.shape, BF16)] * 2,
        in_specs=[VMEM_SPEC] * 7 + [ANY_SPEC],
        out_specs=[VMEM_SPEC] * 2,
        scratch_shapes=mixer_scratch(residual, queries, heads, out_weight),
        compiler_params=pltpu.CompilerParams(
            collective_id=0, has_side_effects=True, vmem_limit_bytes=48 << 20
        ),
        name="mixer",
    )(queries, keys, values, offsets.T, docs[None, :], residual, gain[None, :], out_weight)


def slot_row(ids, tp, rows):
    tok = ids.shape[1]
    group = jnp.broadcast_to((ids[:1, :] // 2).astype(F32), (8, tok)).astype(BF16)
    at = lax.broadcasted_iota(jnp.int32, (tok, 128), 0)
    lane = lax.broadcasted_iota(jnp.int32, (tok, 128), 1)
    pick = jnp.where(at == lane + tp * rows, 1.0, 0.0).astype(BF16)
    mine = jnp.dot(group, pick, preferred_element_type=F32)
    before_at = lax.broadcasted_iota(jnp.int32, (128, 128), 0)
    before_lane = lax.broadcasted_iota(jnp.int32, (128, 128), 1)
    before = jnp.where(before_at < before_lane, 1.0, 0.0).astype(BF16)
    ones = jnp.dot(mine.astype(BF16), before, preferred_element_type=F32)
    token = lax.broadcasted_iota(jnp.int32, (8, 128), 1).astype(F32)
    slot = jnp.where(mine > 0.5, ones + rows // 2, token - ones)
    return slot[:1, :rows]


def experts_kernel(
    chips,
    w_copies, w_copy, res_copy, attended, drain_kv,
    mixed_ref, res_ref, gain_ref, ids_ref, group_ref, expert_ref,
    out_ref,
    w_buf, sums, sums_in, a_down_in, a_up_in, a_send, a_recv, a_sems,
    router_ref, gate, up, down, rows, y_out, part, partner_in, x_in, down_in, up_in, y_in, total,
    out_buf, out_sem, y_sem, rows_recv, fan_recv, line_send, bulk, p_recv, xr_recv,
):
    sp = lax.axis_index("sp")
    tp = lax.axis_index("tp")
    y, x = sp // 2, sp % 2
    chip, core = tp // 2, tp % 2
    partner = (sp, tp + 1 - 2 * core)
    x_peer = (sp + 1 - 2 * x, tp)
    y_peer = (lax.rem(sp + 2, 4), tp)
    below, above = (sp, tp - 2), (sp, tp + 2)
    has_below, has_above = chip > 0, chip < chips - 1
    row_count, width = res_ref.shape
    half_rows = row_count // 2
    half_width = width // 2

    slots = slot_row(ids_ref[...], tp, row_count)
    slot_iota = lax.broadcasted_iota(jnp.int32, (half_rows, row_count), 0)

    def selection(group):
        wanted = (slot_iota + group * half_rows).astype(F32)
        return jnp.where(wanted == slots, 1.0, 0.0).astype(BF16)

    sel_own, sel_other = selection(y), selection(1 - y)
    router_ref[...] = jnp.zeros_like(router_ref)
    router_ref[0:2, :] = group_ref[...].astype(F32)
    router_ref[2:6, :] = expert_ref[...].astype(F32)

    def span(h):
        return columns(h, width)

    def y_copy(h):
        return remote(
            y_out.at[:, span(h)], rows.at[x, chip, core, y, :, span(h)], y_sem.at[5 + h],
            rows_recv.at[x, chip, y, h], y_peer,
        )

    def piece_copy(xs, z, s, h, send, device):
        piece = rows.at[xs, z, core, s, :, span(h)]
        return remote(piece, piece, send, rows_recv.at[xs, z, s, h], device)

    def fan_copy(xs, z, s, h):
        piece = rows.at[xs, z, core, s, :, span(h)]
        return remote(piece, piece, bulk.at[0], fan_recv.at[z], partner)

    def line_piece(z, s, h, up_ok, down_ok, act):
        @pl.when(down_ok)
        def _():
            act(piece_copy(x, z, s, h, line_send.at[z, 0], below))

        @pl.when(up_ok)
        def _():
            act(piece_copy(x, z, s, h, line_send.at[z, 1], above))

        act(piece_copy(x, z, s, h, bulk.at[1], x_peer))
        act(fan_copy(x, z, s, h))

    def begin(copy):
        copy.start()

    def arrived(xs, z, s, h):
        piece_copy(xs, z, s, h, y_sem.at[0], x_peer).wait_recv()

    def own_rest(s):
        for h in range(2):
            arrived(x, chip, s, h)
            line_piece(chip, s, h, has_above, has_below, begin)

    def line_pieces(distance, s, act, wait):
        for h in range(2):

            @pl.when(chip - distance >= 0)
            def _():
                if wait:
                    arrived(x, chip - distance, s, h)
                line_piece(chip - distance, s, h, has_above, chip < 0, act)

            @pl.when(chip + distance < chips)
            def _():
                if wait:
                    arrived(x, chip + distance, s, h)
                line_piece(chip + distance, s, h, chip < 0, has_below, act)

    def at_distance(distance, body):
        if distance == 0:
            body(chip)
            return

        @pl.when(chip - distance >= 0)
        def _():
            body(chip - distance)

        @pl.when(chip + distance < chips)
        def _():
            body(chip + distance)

    def cross(z, s, act, wait):
        for h in range(2):
            if wait:
                arrived(1 - x, z, s, h)
            act(fan_copy(1 - x, z, s, h))

    def a_copy(z, h):
        cols = columns(h, width)
        return remote(
            sums.at[1 - core, z, :, :, cols], sums_in.at[z, :, :, cols], a_send.at[0],
            a_recv.at[z, h], partner,
        )

    w_copy.wait()
    for h in range(2):
        project(attended, w_buf, sums, chips, half_rows, h * half_width, (h + 1) * half_width)
        for z in range(chips):
            a_copy(z, h).start()

    def fold(dest, p):
        if p < 2:
            cols = columns(p, width)
            a_copy(dest, p).wait_recv()
            sums[core, dest, :, :, cols] = (
                sums[core, dest, :, :, cols].astype(F32) + sums_in[dest, :, :, cols].astype(F32)
            ).astype(BF16)

    mix = Line(
        chips, chip, sp, tp, lambda z: sums.at[core, z],
        lambda z, p: sums.at[core, z, p // 2, :, columns(p, width)],
        a_down_in, a_up_in, a_sems,
    )

    def settle():
        for p in range(PIECES):
            mix.own(p, fold)
        added = sums[core, chip].reshape(row_count, width).astype(F32)
        mixed = (res_ref[...].astype(F32) + added).astype(BF16)
        mixed_ref[...] = mixed
        mixed_f = mixed.astype(F32)
        scaling = lax.rsqrt(jnp.mean(mixed_f * mixed_f, axis=1, keepdims=True) + 1e-06)
        normed = (mixed_f * scaling * gain_ref[...]).astype(BF16)
        for h in range(2):
            cols = slice(h * half_width, (h + 1) * half_width)
            y_out[:, cols] = jnp.dot(
                sel_other, normed[:, cols], preferred_element_type=F32
            ).astype(BF16)
            y_copy(h).start()
            rows[x, chip, core, y, :, cols] = jnp.dot(
                sel_own, normed[:, cols], preferred_element_type=F32
            ).astype(BF16)
            line_piece(chip, y, h, has_above, has_below, begin)

    def p_copy(z):
        return remote(part.at[z, 1 - core], partner_in.at[z], bulk.at[2], p_recv.at[z], partner)

    def xr_copy(z, s):
        return remote(
            part.at[z, core, 1 - x, s], x_in.at[z, s], bulk.at[3], xr_recv.at[z, s], x_peer
        )

    lanes = lax.broadcasted_iota(jnp.int32, (1, router_ref.shape[0]), 1)

    def signed(plus, minus):
        return jnp.where(lanes == plus, 1.0, 0.0) - jnp.where(lanes == minus, 1.0, 0.0)

    group_sign = signed(y, 1 - y)
    expert_sign = signed(2 + sp, 2 + sp + 1 - 2 * x)

    def expert(z):
        fanned = rows.at[:, z, 1 - core]
        remote(fanned, fanned, bulk.at[0], fan_recv.at[z], partner).wait_recv()
        block = rows[:, z].reshape(8 * half_rows, width)
        logits = lax.dot_general(
            block, router_ref[...].astype(BF16), (((1,), (1,)), ((), ())), preferred_element_type=F32
        )
        route = jax.nn.sigmoid(
            jnp.sum(logits * group_sign, axis=1, keepdims=True)
        ) * jax.nn.sigmoid(jnp.sum(logits * expert_sign, axis=1, keepdims=True))
        gated = jnp.dot(block, gate[...], preferred_element_type=F32)
        raised = jnp.dot(block, up[...], preferred_element_type=F32)
        hidden = (jax.nn.silu(gated) * raised).astype(BF16)
        tile = 1024
        for n in range(width // tile):
            cols = slice(n * tile, (n + 1) * tile)
            out = jnp.dot(hidden, down[:, cols], preferred_element_type=F32) * route
            out = out.astype(BF16)
            for xs in range(2):
                for c in range(2):
                    for s in range(2):
                        at = ((xs * 2 + c) * 2 + s) * half_rows
                        part[z, c, xs, s, :, cols] = out[at : at + half_rows]
        p_copy(z).start()

    halves = (1 - y, y)

    def send_x(z, s):
        xr_copy(z, s).start()

    def join_cores(z, send=True):
        p_copy(z).wait_recv()
        for xs in (1 - x, x):
            for s in halves:
                part[z, core, xs, s] = (
                    part[z, core, xs, s].astype(F32) + partner_in[z, xs, s].astype(F32)
                ).astype(BF16)
                if xs is not x and send:
                    xr_copy(z, s).start()

    def join_x(z, piece):
        s = halves[piece // 2]
        if piece % 2 == 0:
            xr_copy(z, s).wait_recv()
            part[z, core, x, s] = (
                part[z, core, x, s].astype(F32) + x_in[z, s].astype(F32)
            ).astype(BF16)

    def back_copy(n):
        cols = columns(n, width)
        return remote(
            part.at[chip, core, x, 1 - y, :, cols], y_in.at[:, cols], y_sem.at[1 + n],
            y_sem.at[3 + n], y_peer,
        )

    def finished(piece):
        cols = columns(piece, width)
        if piece < 2:
            back_copy(piece).start()
        else:
            sums = lax.dot_general(
                sel_own, part[chip, core, x, y, :, cols], (((0,), (0,)), ((), ())),
                preferred_element_type=F32,
            )
            total[:, cols] = mixed_ref[:, cols].astype(F32) + sums

    for distance in range(chips - 1, 0, -1):
        mix.send(chip - distance, chip + distance, range(PIECES), fold)
    res_copy.wait()

    def cross_all(distance, s):
        at_distance(distance, lambda z: cross(z, s, begin, True))

    @pl.when(y == 0)
    def _():
        settle()

    @pl.when(y == 1)
    def _():
        own_rest(0)
        settle()

    line_pieces(1, 0, begin, True)

    @pl.when(y == 1)
    def _():
        line_pieces(1, 1, begin, True)

    line_pieces(2, 0, begin, True)

    @pl.when(y == 0)
    def _():
        own_rest(1)
        line_pieces(1, 1, begin, True)

    cross_all(0, 0)
    cross_all(1, 0)
    cross_all(0, 1)
    for copy in w_copies:
        copy.wait()
    is_end = (chip == 0) | (chip == chips - 1)

    at_distance(0, expert)
    line_pieces(2, 1, begin, True)
    cross_all(1, 1)
    at_distance(1, expert)
    at_distance(0, lambda z: join_cores(z, False))
    for s in range(2):
        line_pieces(3, s, begin, True)
        cross_all(2, s)
    at_distance(1, join_cores)
    at_distance(2, expert)

    @pl.when(is_end)
    def _():
        send_x(chip, 1 - y)

    for s in range(2):
        cross_all(3, s)
    at_distance(2, lambda z: join_cores(z, False))

    @pl.when(jnp.logical_not(is_end))
    def _():
        for s in halves:
            at_distance(2, lambda z: send_x(z, s))
        send_x(chip, 1 - y)

    at_distance(3, expert)
    at_distance(3, join_cores)

    @pl.when(is_end)
    def _():
        for s in halves:
            at_distance(2, lambda z: send_x(z, s))

    send_x(chip, y)
    back = Line(
        chips, chip, sp, tp, lambda z: part.at[z, core, x],
        lambda z, p: part.at[z, core, x, halves[p // 2], :, columns(p, width)],
        down_in, up_in, a_sems,
    )
    def back_turn(distance, mine):
        back.send(
            jnp.where(mine, chip - distance, -1), jnp.where(mine, chip + distance, chips),
            range(PIECES), join_x,
        )

    def end(copy):
        copy.wait_send()

    def drain_dispatch():
        for h in range(2):
            end(y_copy(h))
        end(remote(sums.at[1 - core], sums_in, a_send.at[0], a_recv.at[0, 0], partner))
        mine = rows.at[:, :, core]
        end(remote(mine, mine, bulk.at[0], fan_recv.at[0], partner))
        crossed = rows.at[x, :, core]
        end(remote(crossed, crossed, bulk.at[1], fan_recv.at[0], x_peer))
        for z in range(chips):
            chunk = rows.at[x, z, core]

            @pl.when((z >= chip) & has_below)
            def _():
                end(remote(chunk, chunk, line_send.at[z, 0], fan_recv.at[0], below))

            @pl.when((z <= chip) & has_above)
            def _():
                end(remote(chunk, chunk, line_send.at[z, 1], fan_recv.at[0], above))

        end(remote(part.at[:, 1 - core], partner_in, bulk.at[2], p_recv.at[0], partner))
        drain_kv()

    mix.drain()
    back_turn(1, is_end)
    drain_dispatch()
    for distance in range(chips - 1, 1, -1):
        back_turn(distance, True)
    back_turn(1, jnp.logical_not(is_end))
    for p in range(PIECES):
        back.own(p, join_x)
        finished(p)
    def out_copy(n):
        cols = columns(n, width)
        return pltpu.make_async_copy(out_buf.at[:, cols], out_ref.at[:, cols], out_sem.at[n])

    for n in range(2):
        cols = columns(n, width)
        back_copy(n).wait_recv()
        returned = lax.dot_general(
            sel_other, y_in[:, cols], (((0,), (0,)), ((), ())), preferred_element_type=F32
        )
        out_buf[:, cols] = (total[:, cols] + returned).astype(BF16)
        out_copy(n).start()

    for n in range(2):
        end(back_copy(n))
    end(remote(part.at[:, core, 1 - x], x_in, bulk.at[3], xr_recv.at[0, 0], x_peer))
    back.drain()
    for n in range(2):
        out_copy(n).wait()


def layer_kernel(
    sp_count, chips, heads, mixer_count,
    q_hbm, k_hbm, v_hbm, res_hbm, w_hbm, gate_hbm, up_hbm, down_hbm,
    off_ref, doc_ref, gain_ref, ids_ref, group_ref, expert_ref,
    out_ref,
    q_ref, k_ref, v_ref, res_ref, mixed_ref, load_sem, weight_sem, router_ref,
    gate, up, down,
    *scratch,
):
    loads = [
        pltpu.make_async_copy(src, dst, load_sem.at[n])
        for n, (src, dst) in enumerate(
            ((k_hbm, k_ref), (v_hbm, v_ref), (q_hbm, q_ref), (res_hbm, res_ref))
        )
    ]
    weights = [
        pltpu.make_async_copy(src.at[0], dst, weight_sem.at[n])
        for n, (src, dst) in enumerate(((gate_hbm, gate), (up_hbm, up), (down_hbm, down)))
    ]
    for copy in loads[:3]:
        copy.start()
    (
        meta_ref, doc_col, k_buf, v_buf, m_buf, acc, carry, w_buf, sums, sums_in, a_down_in, a_up_in,
        w_sem, kv_send, kv_recv, a_send, a_recv,
    ) = scratch[: mixer_count - 4]
    a_sems = scratch[mixer_count - 4 : mixer_count]
    w_copy = pltpu.make_async_copy(w_hbm, w_buf, w_sem)
    attended, drain_kv = attention(
        sp_count, chips, heads, True, loads[:3], [w_copy, loads[3]] + weights,
        q_ref, k_ref, v_ref, off_ref, doc_ref,
        meta_ref, doc_col, k_buf, v_buf, m_buf, acc, carry, kv_send, kv_recv,
    )
    experts_kernel(
        chips, weights, w_copy, loads[3], attended, drain_kv,
        mixed_ref, res_ref, gain_ref, ids_ref, group_ref, expert_ref, out_ref,
        w_buf, sums, sums_in, a_down_in, a_up_in, a_send, a_recv, a_sems,
        router_ref, gate, up, down, *scratch[mixer_count:],
    )


def pair_layer(
    residual, queries, keys, values, offsets, docs, out_weight, gain,
    expert_ids, group_router, expert_router, gate, up, down,
):
    chips = lax.axis_size("tp") // 2
    rows, width = residual.shape
    heads = offsets.shape[1]
    mixer_parts = mixer_scratch(residual, queries, heads, out_weight)
    half_rows = rows // 2
    units = gate.shape[2]
    half = (chips, 2, half_rows, width)
    quarter = (chips, PIECES, half_rows, width // 2)
    dma = pltpu.SemaphoreType.DMA
    return pl.pallas_call(
        functools.partial(
            layer_kernel, lax.axis_size("sp"), chips, heads, len(mixer_parts)
        ),
        out_shape=jax.ShapeDtypeStruct((rows, width), BF16),
        in_specs=[ANY_SPEC] * 8 + [VMEM_SPEC] * 6,
        out_specs=ANY_SPEC,
        scratch_shapes=[
            pltpu.VMEM(queries.shape, BF16),
            pltpu.VMEM(keys.shape, BF16),
            pltpu.VMEM(values.shape, BF16),
            pltpu.VMEM((rows, width), BF16),
            pltpu.VMEM((rows, width), BF16),
            dma((4,)),
            dma((3,)),
            pltpu.VMEM((8, width), F32),
            pltpu.VMEM((width, units), BF16),
            pltpu.VMEM((width, units), BF16),
            pltpu.VMEM((units, width), BF16),
        ]
        + mixer_parts
        + [
            pltpu.VMEM((2, chips, 2, 2, half_rows, width), BF16),
            pltpu.VMEM((half_rows, width), BF16),
            pltpu.VMEM((chips, 2, 2, 2, half_rows, width), BF16),
            pltpu.VMEM((chips, 2, 2, half_rows, width), BF16),
            pltpu.VMEM(half, BF16),
            pltpu.VMEM(quarter, BF16),
            pltpu.VMEM(quarter, BF16),
            pltpu.VMEM((half_rows, width), BF16),
            pltpu.VMEM((rows, width), F32),
            pltpu.VMEM((rows, width), BF16),
            dma((2,)),
            dma((7,)),
            dma((2, chips, 2, 2)),
            dma((chips,)),
            dma((chips, 2)),
            dma((4,)),
            dma((chips,)),
            dma((chips, 2)),
        ],
        compiler_params=pltpu.CompilerParams(
            collective_id=1, has_side_effects=True, vmem_limit_bytes=60 << 20
        ),
        name="layer",
    )(
        queries, keys, values, residual, out_weight, gate, up, down,
        offsets.T, docs[None, :], gain[None, :], expert_ids.T, group_router.T, expert_router.T,
    )


def per_device(
    residual_in,
    queries,
    keys,
    values,
    break_offset,
    doc_ids,
    out_weight,
    norm_gain,
    group_router,
    expert_router,
    expert_ids,
    gate_weight,
    up_weight,
    down_weight,
):
    tok_dev = queries.shape[0]
    sp_count = lax.axis_size("sp")
    tp_count = lax.axis_size("tp")
    tp_rank = lax.axis_index("tp")
    width = residual_in.shape[1]
    rows_dev = tok_dev // tp_count
    chosen = lax.dynamic_slice_in_dim(expert_ids, tp_rank * rows_dev, rows_dev, 0)
    expert_count = sp_count * gate_weight.shape[0]
    group_size = expert_count // GROUPS
    if sp_count == 4 and gate_weight.shape[0] == 1 and rows_dev % 32 == 0:
        return pair_layer(
            residual_in, queries, keys, values, break_offset, doc_ids, out_weight, norm_gain,
            expert_ids, group_router, expert_router, gate_weight, up_weight, down_weight,
        )
    mixed_stream, normed = mixer(
        residual_in, queries, keys, values, break_offset, doc_ids, out_weight, norm_gain
    )
    routes = route_weights(normed, group_router, expert_router, chosen, group_size)
    slots = 2 * rows_dev // expert_count
    slot_ids = slot_table(chosen, expert_count, slots)
    sent = dispatch(normed, slot_ids, expert_count * slots).reshape(expert_count, slots, width)
    fanned = lax.all_gather(
        lax.all_to_all(sent, "sp", split_axis=0, concat_axis=0, tiled=True),
        "tp",
        axis=0,
        tiled=True,
    )
    partial_out = expert_rows(
        fanned.reshape(-1, width), gate_weight[0], up_weight[0], down_weight[0]
    )
    unit_total = lax.psum_scatter(
        partial_out.reshape(fanned.shape), "tp", scatter_dimension=0, tiled=True
    ).astype(jnp.float32)
    returned = lax.all_to_all(
        unit_total.astype(jnp.bfloat16), "sp", split_axis=0, concat_axis=0, tiled=True
    )
    expert_out = jnp.take(returned.reshape(-1, width), slot_ids.reshape(-1), axis=0).reshape(
        rows_dev, 2, width
    )
    mixture = jnp.sum(routes[:, :, None] * expert_out.astype(jnp.float32), axis=1)
    return (mixed_stream.astype(jnp.float32) + mixture).astype(jnp.bfloat16)


def solution(mesh):
    return jax.shard_map(
        per_device,
        mesh=mesh,
        in_specs=(
            P(("sp", "tp"), None),
            P("sp", "tp"),
            P("sp", "tp"),
            P("sp", "tp"),
            P("sp", "tp"),
            P("sp"),
            P("tp", None),
            P(),
            P(),
            P(),
            P("sp", None),
            P("sp", None, "tp"),
            P("sp", None, "tp"),
            P("sp", "tp", None),
        ),
        out_specs=P(("sp", "tp"), None),
        check_vma=False,
    )
```

```python
import functools

import jax
import jax.numpy as jnp
from jax import lax
from jax.experimental import pallas as pl
from jax.experimental.pallas import tpu as pltpu
from jax.sharding import PartitionSpec as P

HEAD_DIM = 64
PIECES = 4
GROUPS = 2


def route_weights(normed, group_router, expert_router, chosen, group_size):
    group_logits = jnp.dot(normed, group_router, preferred_element_type=jnp.float32)
    expert_logits = jnp.dot(normed, expert_router, preferred_element_type=jnp.float32)
    chosen_group = chosen[:, 0] // group_size
    margin = group_logits[:, 0] - group_logits[:, 1]
    own_margin = jnp.where(chosen_group == 0, margin, -margin)
    experts_iota = jnp.arange(expert_logits.shape[1], dtype=jnp.int32)
    picked = jnp.sum(
        jnp.where(
            chosen[:, :, None] == experts_iota[None, None, :],
            expert_logits[:, None, :],
            jnp.float32(0.0),
        ),
        axis=2,
    )
    return jax.nn.sigmoid(own_margin)[:, None] * jax.nn.sigmoid(picked - picked[:, ::-1])


def slot_table(chosen, expert_count, slots):
    flat_ids = chosen.reshape(-1)
    onehot = (flat_ids[:, None] == jnp.arange(expert_count, dtype=jnp.int32)[None, :]).astype(
        jnp.int32
    )
    before = jnp.cumsum(onehot, axis=0) - onehot
    ranks = jnp.sum(before * onehot, axis=1)
    return (flat_ids * slots + ranks).reshape(chosen.shape)


def dispatch(normed, slot_ids, total_slots):
    flat_slots = slot_ids.reshape(-1)
    owners = jnp.arange(flat_slots.shape[0], dtype=jnp.int32) // 2
    slot_iota = jnp.arange(total_slots, dtype=jnp.int32)
    token_of_slot = jnp.sum(
        jnp.where(slot_iota[:, None] == flat_slots[None, :], owners[None, :], 0), axis=1
    )
    return jnp.take(normed, token_of_slot, axis=0)


def expert_rows(row_block, gate_part, up_part, down_part):
    gate_val = jnp.dot(row_block, gate_part, preferred_element_type=jnp.float32)
    up_val = jnp.dot(row_block, up_part, preferred_element_type=jnp.float32)
    hidden = (jax.nn.silu(gate_val) * up_val).astype(jnp.bfloat16)
    return jnp.dot(hidden, down_part, preferred_element_type=jnp.float32).astype(jnp.bfloat16)


MESH_ID = pl.DeviceIdType.MESH
VMEM_SPEC = pl.BlockSpec(memory_space=pltpu.VMEM)
ANY_SPEC = pl.BlockSpec(memory_space=pl.ANY)
F32 = jnp.float32
BF16 = jnp.bfloat16


def remote(src, dst, send_sem, recv_sem, device):
    return pltpu.make_async_remote_copy(
        src_ref=src, dst_ref=dst, send_sem=send_sem, recv_sem=recv_sem,
        device_id=device, device_id_type=MESH_ID,
    )


def columns(piece, width):
    return pl.ds((piece % 2) * (width // 2), width // 2)


def greet(device):
    pl.semaphore_signal(
        pltpu.get_barrier_semaphore(), inc=1, device_id=device, device_id_type=MESH_ID
    )


class Line:
    def __init__(self, chips, chip, sp, tp, whole, block, down_in, up_in, sems):
        self.chips, self.chip, self.whole, self.block = chips, chip, whole, block
        down_send, down_recv, up_send, up_recv = sems
        self.legs = (
            (down_in, down_send, down_recv, (sp, tp - 2), chip < chips - 1),
            (up_in, up_send, up_recv, (sp, tp + 2), chip > 0),
        )

    def copy(self, leg, dest, p, device):
        inbox, send, recv = leg[:3]
        return remote(
            self.block(dest, p), inbox.at[dest, p], send.at[dest], recv.at[dest, p], device
        )

    def gather(self, leg, dest, p, device):
        @pl.when(leg[4])
        def _():
            self.copy(leg, dest, p, device).wait_recv()
            piece = self.block(dest, p)
            piece[...] = (piece[...].astype(F32) + leg[0][dest, p].astype(F32)).astype(BF16)

    def send(self, below, above, pieces, ready):
        chip, chips = self.chip, self.chips
        for p in pieces:
            for leg, dest, valid in (
                (self.legs[0], below, (below >= 0) & (below < chip)),
                (self.legs[1], above, (above > chip) & (above < chips)),
            ):

                @pl.when(valid)
                def _():
                    ready(dest, p)
                    self.gather(leg, dest, p, leg[3])
                    self.copy(leg, dest, p, leg[3]).start()

    def own(self, p, ready):
        ready(self.chip, p)
        for leg in self.legs:
            self.gather(leg, self.chip, p, leg[3])

    def drain(self):
        for dest in range(self.chips):
            for leg, sent in ((self.legs[0], dest < self.chip), (self.legs[1], dest > self.chip)):

                @pl.when(sent)
                def _():
                    chunk = self.whole(dest)
                    remote(
                        chunk, chunk, leg[1].at[dest], leg[2].at[dest, 0], leg[3]
                    ).wait_send()


def attention(
    sp_count, chips, heads, relay, tables, loads, later_loads,
    q_ref, k_ref, v_ref, off_ref, doc_ref,
    meta_ref, doc_col, k_buf, v_buf, m_buf, acc, carry, kv_send, kv_recv,
):
    sp = lax.axis_index("sp")
    tp = lax.axis_index("tp")
    chip = tp // 2
    core = tp % 2
    partner = tp + 1 - 2 * core
    tok, att = q_ref.shape
    for j in range(1, sp_count):
        greet((lax.rem(sp + j, sp_count), tp))
    greet((sp, partner))

    @pl.when(chip > 0)
    def _():
        greet((sp, tp - 2))

    @pl.when(chip < chips - 1)
    def _():
        greet((sp, tp + 2))

    expect = sp_count + jnp.where(chip > 0, 1, 0) + jnp.where(chip < chips - 1, 1, 0)
    for copy in tables:
        copy.wait()
    docs = doc_ref[...].astype(F32)
    meta_ref[...] = jnp.zeros_like(meta_ref)
    meta_ref[0:heads, :] = off_ref[...].astype(F32)
    meta_ref[heads : heads + 1, :] = docs
    doc_col[...] = jnp.broadcast_to(docs, (128, tok)).T[:, :1]
    for copy in loads:
        copy.wait()
    pl.semaphore_wait(pltpu.get_barrier_semaphore(), expect)

    def kv_copies(j, target):
        return [
            remote(src, buf.at[j - 1], kv_send.at[j - 1, n], kv_recv.at[j - 1, n], (target, tp))
            for n, (src, buf) in enumerate(((k_ref, k_buf), (v_ref, v_buf), (meta_ref, m_buf)))
        ]

    def sends(act):
        for j in range(1, sp_count):
            keys, *others = kv_copies(j, sp + j)
            direct = sp + j < sp_count

            @pl.when(direct & (sp + j != sp_count - 1 - sp) if relay else direct)
            def _():
                act(keys)

            @pl.when(direct)
            def _():
                for copy in others:
                    act(copy)

    def relayed():
        slot = 2 * x_peer - sp_count
        return remote(
            k_buf.at[1], k_buf.at[slot], kv_send.at[2, 0], kv_recv.at[slot, 0], (x_peer, tp)
        )

    x_peer = sp + 1 - 2 * (sp % 2)
    sends(lambda copy: copy.start())

    for copy in later_loads:
        copy.start()

    row = lax.broadcasted_iota(jnp.int32, (tok, tok), 0)
    col = lax.broadcasted_iota(jnp.int32, (tok, tok), 1)
    later = jnp.where(row > col, 1.0, 0.0).astype(BF16)
    lane = lax.broadcasted_iota(jnp.int32, (tok, att), 1) // HEAD_DIM
    acc[...] = jnp.zeros_like(acc)
    carry[...] = jnp.zeros_like(carry)

    def attend_block(keys, vals, meta, own):
        live = doc_col[...] == meta[heads : heads + 1, :]
        if own:
            live = live & (col < row)
        for h in range(heads):
            queries = jnp.where(lane == h, q_ref[...], jnp.zeros((), BF16)) * jnp.asarray(
                HEAD_DIM ** (-0.5), BF16
            )
            scores = lax.dot_general(
                queries, keys, (((1,), (1,)), ((), ())), preferred_element_type=F32
            ) + meta[h : h + 1, :]
            soft = jnp.maximum(scores, 0.0) + jnp.log(1.0 + jnp.exp(-jnp.abs(scores)))
            stay = jnp.where(live, -soft, 0.0)
            high = stay.astype(BF16)
            low = (stay - high.astype(F32)).astype(BF16)
            within = jnp.dot(high, later, preferred_element_type=F32) + jnp.dot(
                low, later, preferred_element_type=F32
            )
            before = carry[h]
            weights = jnp.where(
                live, jnp.exp(scores - soft + within + before), 0.0
            ).astype(BF16)
            out = jnp.dot(weights, vals, preferred_element_type=F32)
            acc[...] += jnp.where(lane == h, out, 0.0)
            carry[h] = before + within[:, :1] + stay[:, :1]

    attend_block(k_ref[...], v_ref[...], meta_ref[...], True)

    if relay:

        @pl.when(sp >= 2)
        def _():
            kv_copies(2, sp)[0].wait_recv()
            relayed().start()

    def earlier(j, unused):
        @pl.when(sp - j >= 0)
        def _():
            keys, *others = kv_copies(j, sp)

            @pl.when((sp < 2) | (j != 2) if relay else True)
            def _():
                keys.wait_recv()

            for copy in others:
                copy.wait_recv()
            attend_block(k_buf[j - 1], v_buf[j - 1], m_buf[j - 1], False)

        return unused

    lax.fori_loop(1, sp_count, earlier, 0)

    def drain():
        sends(lambda copy: copy.wait_send())
        if relay:

            @pl.when(sp >= 2)
            def _():
                relayed().wait_send()

    return acc[...].astype(BF16), drain


def project(attended, w_buf, part, chips, half_rows, first, last):
    tile = 512
    for n in range(first // tile, last // tile):
        cols = slice(n * tile, (n + 1) * tile)
        product = jnp.dot(attended, w_buf[:, cols], preferred_element_type=F32).astype(BF16)
        for z in range(chips):
            for c in range(2):
                for s in range(2):
                    at = ((z * 2 + c) * 2 + s) * half_rows
                    part[c, z, s, :, cols] = product[at : at + half_rows]


def mixer_kernel(
    sp_count, chips, heads,
    q_ref, k_ref, v_ref, off_ref, doc_ref, res_ref, gain_ref, w_hbm,
    mixed_ref, normed_ref,
    meta_ref, doc_col, k_buf, v_buf, m_buf, acc, carry, w_buf, part, partner_in, down_in, up_in,
    w_sem, kv_send, kv_recv, p_send, p_recv, down_send, down_recv, up_send, up_recv,
):
    sp = lax.axis_index("sp")
    tp = lax.axis_index("tp")
    chip = tp // 2
    core = tp % 2
    width = res_ref.shape[1]
    half_rows = res_ref.shape[0] // 2
    w_copy = pltpu.make_async_copy(w_hbm, w_buf, w_sem)
    attended, drain_kv = attention(
        sp_count, chips, heads, False, (), (), (w_copy,),
        q_ref, k_ref, v_ref, off_ref, doc_ref,
        meta_ref, doc_col, k_buf, v_buf, m_buf, acc, carry, kv_send, kv_recv,
    )
    w_copy.wait()
    project(attended, w_buf, part, chips, half_rows, 0, width)

    def p_copy(z):
        return remote(
            part.at[1 - core, z], partner_in.at[z], p_send.at[z], p_recv.at[z, 0],
            (sp, tp + 1 - 2 * core),
        )

    for z in range(chips):
        p_copy(z).start()
    for z in range(chips):
        p_copy(z).wait_recv()
        part[core, z] = (part[core, z].astype(F32) + partner_in[z].astype(F32)).astype(BF16)
    line = Line(
        chips, chip, sp, tp, lambda z: part.at[core, z],
        lambda z, p: part.at[core, z, p // 2, :, columns(p, width)],
        down_in, up_in, (down_send, down_recv, up_send, up_recv),
    )
    for distance in range(chips - 1, 0, -1):
        line.send(chip - distance, chip + distance, range(PIECES), lambda dest, p: None)
    for p in range(PIECES):
        line.own(p, lambda dest, p: None)
    total = part[core, chip].reshape(res_ref.shape).astype(F32)
    mixed = (res_ref[...].astype(F32) + total).astype(BF16)
    mixed_ref[...] = mixed
    mixed_f = mixed.astype(F32)
    scaling = lax.rsqrt(jnp.mean(mixed_f * mixed_f, axis=1, keepdims=True) + 1e-06)
    normed_ref[...] = (mixed_f * scaling * gain_ref[...]).astype(BF16)
    for z in range(chips):
        p_copy(z).wait_send()
    line.drain()
    drain_kv()


def mixer_scratch(residual, queries, heads, out_weight):
    sp_count = lax.axis_size("sp")
    chips = lax.axis_size("tp") // 2
    rows, width = residual.shape
    tok, att = queries.shape
    others = max(sp_count - 1, 1)
    half = (chips, 2, rows // 2, width)
    quarter = (chips, PIECES, rows // 2, width // 2)
    dma = pltpu.SemaphoreType.DMA
    meta_shape = (heads + 1 + -(heads + 1) % 8, tok)
    return [
        pltpu.VMEM(meta_shape, F32),
        pltpu.VMEM((tok, 1), F32),
        pltpu.VMEM((others, tok, att), BF16),
        pltpu.VMEM((others, tok, att), BF16),
        pltpu.VMEM((others,) + meta_shape, F32),
        pltpu.VMEM((tok, att), F32),
        pltpu.VMEM((heads, tok, 1), F32),
        pltpu.VMEM(out_weight.shape, BF16),
        pltpu.VMEM((2,) + half, BF16),
        pltpu.VMEM(half, BF16),
        pltpu.VMEM(quarter, BF16),
        pltpu.VMEM(quarter, BF16),
        dma,
        dma((others, 3)),
        dma((others, 3)),
        dma((chips,)),
        dma((chips, 2)),
    ] + [dma((chips,)), dma((chips, PIECES))] * 2


def mixer(residual, queries, keys, values, offsets, docs, out_weight, gain):
    heads = offsets.shape[1]
    return pl.pallas_call(
        functools.partial(
            mixer_kernel, lax.axis_size("sp"), lax.axis_size("tp") // 2, heads
        ),
        out_shape=[jax.ShapeDtypeStruct(residual.shape, BF16)] * 2,
        in_specs=[VMEM_SPEC] * 7 + [ANY_SPEC],
        out_specs=[VMEM_SPEC] * 2,
        scratch_shapes=mixer_scratch(residual, queries, heads, out_weight),
        compiler_params=pltpu.CompilerParams(
            collective_id=0, has_side_effects=True, vmem_limit_bytes=48 << 20
        ),
        name="mixer",
    )(queries, keys, values, offsets.T, docs[None, :], residual, gain[None, :], out_weight)


def slot_row(ids, tp, rows):
    tok = ids.shape[1]
    group = jnp.broadcast_to((ids[:1, :] // 2).astype(F32), (8, tok)).astype(BF16)
    at = lax.broadcasted_iota(jnp.int32, (tok, 128), 0)
    lane = lax.broadcasted_iota(jnp.int32, (tok, 128), 1)
    pick = jnp.where(at == lane + tp * rows, 1.0, 0.0).astype(BF16)
    mine = jnp.dot(group, pick, preferred_element_type=F32)
    before_at = lax.broadcasted_iota(jnp.int32, (128, 128), 0)
    before_lane = lax.broadcasted_iota(jnp.int32, (128, 128), 1)
    before = jnp.where(before_at < before_lane, 1.0, 0.0).astype(BF16)
    ones = jnp.dot(mine.astype(BF16), before, preferred_element_type=F32)
    token = lax.broadcasted_iota(jnp.int32, (8, 128), 1).astype(F32)
    slot = jnp.where(mine > 0.5, ones + rows // 2, token - ones)
    return slot[:1, :rows]


def experts_kernel(
    chips,
    w_copies, w_copy, res_copy, attended, drain_kv,
    mixed_ref, res_ref, gain_ref, ids_ref, group_ref, expert_ref,
    out_ref,
    w_buf, sums, sums_in, a_down_in, a_up_in, a_send, a_recv, a_sems,
    router_ref, gate, up, down, rows, y_out, part, partner_in, x_in, down_in, up_in, y_in, total,
    out_buf, out_sem, y_sem, rows_recv, fan_recv, line_send, bulk, p_recv, xr_recv,
):
    sp = lax.axis_index("sp")
    tp = lax.axis_index("tp")
    y, x = sp // 2, sp % 2
    chip, core = tp // 2, tp % 2
    partner = (sp, tp + 1 - 2 * core)
    x_peer = (sp + 1 - 2 * x, tp)
    y_peer = (lax.rem(sp + 2, 4), tp)
    below, above = (sp, tp - 2), (sp, tp + 2)
    has_below, has_above = chip > 0, chip < chips - 1
    row_count, width = res_ref.shape
    half_rows = row_count // 2
    half_width = width // 2

    slots = slot_row(ids_ref[...], tp, row_count)
    slot_iota = lax.broadcasted_iota(jnp.int32, (half_rows, row_count), 0)

    def selection(group):
        wanted = (slot_iota + group * half_rows).astype(F32)
        return jnp.where(wanted == slots, 1.0, 0.0).astype(BF16)

    sel_own, sel_other = selection(y), selection(1 - y)
    router_ref[...] = jnp.zeros_like(router_ref)
    router_ref[0:2, :] = group_ref[...].astype(F32)
    router_ref[2:6, :] = expert_ref[...].astype(F32)

    def span(h):
        return columns(h, width)

    def y_copy(h):
        return remote(
            y_out.at[:, span(h)], rows.at[x, chip, core, y, :, span(h)], y_sem.at[5 + h],
            rows_recv.at[x, chip, y, h], y_peer,
        )

    def piece_copy(xs, z, s, h, send, device):
        piece = rows.at[xs, z, core, s, :, span(h)]
        return remote(piece, piece, send, rows_recv.at[xs, z, s, h], device)

    def fan_copy(xs, z, s, h):
        piece = rows.at[xs, z, core, s, :, span(h)]
        return remote(piece, piece, bulk.at[0], fan_recv.at[z], partner)

    def line_piece(z, s, h, up_ok, down_ok, act):
        @pl.when(down_ok)
        def _():
            act(piece_copy(x, z, s, h, line_send.at[z, 0], below))

        @pl.when(up_ok)
        def _():
            act(piece_copy(x, z, s, h, line_send.at[z, 1], above))

        act(piece_copy(x, z, s, h, bulk.at[1], x_peer))
        act(fan_copy(x, z, s, h))

    def begin(copy):
        copy.start()

    def arrived(xs, z, s, h):
        piece_copy(xs, z, s, h, y_sem.at[0], x_peer).wait_recv()

    def own_rest(s):
        for h in range(2):
            arrived(x, chip, s, h)
            line_piece(chip, s, h, has_above, has_below, begin)

    def line_pieces(distance, s, act, wait):
        for h in range(2):

            @pl.when(chip - distance >= 0)
            def _():
                if wait:
                    arrived(x, chip - distance, s, h)
                line_piece(chip - distance, s, h, has_above, chip < 0, act)

            @pl.when(chip + distance < chips)
            def _():
                if wait:
                    arrived(x, chip + distance, s, h)
                line_piece(chip + distance, s, h, chip < 0, has_below, act)

    def at_distance(distance, body):
        if distance == 0:
            body(chip)
            return

        @pl.when(chip - distance >= 0)
        def _():
            body(chip - distance)

        @pl.when(chip + distance < chips)
        def _():
            body(chip + distance)

    def cross(z, s, act, wait):
        for h in range(2):
            if wait:
                arrived(1 - x, z, s, h)
            act(fan_copy(1 - x, z, s, h))

    def a_copy(z, h):
        cols = columns(h, width)
        return remote(
            sums.at[1 - core, z, :, :, cols], sums_in.at[z, :, :, cols], a_send.at[0],
            a_recv.at[z, h], partner,
        )

    w_copy.wait()
    for h in range(2):
        project(attended, w_buf, sums, chips, half_rows, h * half_width, (h + 1) * half_width)
        for z in range(chips):
            a_copy(z, h).start()

    def fold(dest, p):
        if p < 2:
            cols = columns(p, width)
            a_copy(dest, p).wait_recv()
            sums[core, dest, :, :, cols] = (
                sums[core, dest, :, :, cols].astype(F32) + sums_in[dest, :, :, cols].astype(F32)
            ).astype(BF16)

    mix = Line(
        chips, chip, sp, tp, lambda z: sums.at[core, z],
        lambda z, p: sums.at[core, z, p // 2, :, columns(p, width)],
        a_down_in, a_up_in, a_sems,
    )

    def settle():
        for p in range(PIECES):
            mix.own(p, fold)
        added = sums[core, chip].reshape(row_count, width).astype(F32)
        mixed = (res_ref[...].astype(F32) + added).astype(BF16)
        mixed_ref[...] = mixed
        mixed_f = mixed.astype(F32)
        scaling = lax.rsqrt(jnp.mean(mixed_f * mixed_f, axis=1, keepdims=True) + 1e-06)
        normed = (mixed_f * scaling * gain_ref[...]).astype(BF16)
        for h in range(2):
            cols = slice(h * half_width, (h + 1) * half_width)
            y_out[:, cols] = jnp.dot(
                sel_other, normed[:, cols], preferred_element_type=F32
            ).astype(BF16)
            y_copy(h).start()
            rows[x, chip, core, y, :, cols] = jnp.dot(
                sel_own, normed[:, cols], preferred_element_type=F32
            ).astype(BF16)
            line_piece(chip, y, h, has_above, has_below, begin)

    def p_copy(z):
        return remote(part.at[z, 1 - core], partner_in.at[z], bulk.at[2], p_recv.at[z], partner)

    def xr_copy(z, s):
        return remote(
            part.at[z, core, 1 - x, s], x_in.at[z, s], bulk.at[3], xr_recv.at[z, s], x_peer
        )

    lanes = lax.broadcasted_iota(jnp.int32, (1, router_ref.shape[0]), 1)

    def signed(plus, minus):
        return jnp.where(lanes == plus, 1.0, 0.0) - jnp.where(lanes == minus, 1.0, 0.0)

    group_sign = signed(y, 1 - y)
    expert_sign = signed(2 + sp, 2 + sp + 1 - 2 * x)

    def expert(z):
        fanned = rows.at[:, z, 1 - core]
        remote(fanned, fanned, bulk.at[0], fan_recv.at[z], partner).wait_recv()
        block = rows[:, z].reshape(8 * half_rows, width)
        logits = lax.dot_general(
            block, router_ref[...].astype(BF16), (((1,), (1,)), ((), ())), preferred_element_type=F32
        )
        route = jax.nn.sigmoid(
            jnp.sum(logits * group_sign, axis=1, keepdims=True)
        ) * jax.nn.sigmoid(jnp.sum(logits * expert_sign, axis=1, keepdims=True))
        gated = jnp.dot(block, gate[...], preferred_element_type=F32)
        raised = jnp.dot(block, up[...], preferred_element_type=F32)
        hidden = (jax.nn.silu(gated) * raised).astype(BF16)
        tile = 1024
        for n in range(width // tile):
            cols = slice(n * tile, (n + 1) * tile)
            out = jnp.dot(hidden, down[:, cols], preferred_element_type=F32) * route
            out = out.astype(BF16)
            for xs in range(2):
                for c in range(2):
                    for s in range(2):
                        at = ((xs * 2 + c) * 2 + s) * half_rows
                        part[z, c, xs, s, :, cols] = out[at : at + half_rows]
        p_copy(z).start()

    halves = (1 - y, y)

    def send_x(z, s):
        xr_copy(z, s).start()

    def join_cores(z, send=True):
        p_copy(z).wait_recv()
        for xs in (1 - x, x):
            for s in halves:
                part[z, core, xs, s] = (
                    part[z, core, xs, s].astype(F32) + partner_in[z, xs, s].astype(F32)
                ).astype(BF16)
                if xs is not x and send:
                    xr_copy(z, s).start()

    def join_x(z, piece):
        s = halves[piece // 2]
        if piece % 2 == 0:
            xr_copy(z, s).wait_recv()
            part[z, core, x, s] = (
                part[z, core, x, s].astype(F32) + x_in[z, s].astype(F32)
            ).astype(BF16)

    def back_copy(n):
        cols = columns(n, width)
        return remote(
            part.at[chip, core, x, 1 - y, :, cols], y_in.at[:, cols], y_sem.at[1 + n],
            y_sem.at[3 + n], y_peer,
        )

    def finished(piece):
        cols = columns(piece, width)
        if piece < 2:
            back_copy(piece).start()
        else:
            sums = lax.dot_general(
                sel_own, part[chip, core, x, y, :, cols], (((0,), (0,)), ((), ())),
                preferred_element_type=F32,
            )
            total[:, cols] = mixed_ref[:, cols].astype(F32) + sums

    for distance in range(chips - 1, 0, -1):
        mix.send(chip - distance, chip + distance, range(PIECES), fold)
    res_copy.wait()

    def cross_all(distance, s):
        at_distance(distance, lambda z: cross(z, s, begin, True))

    @pl.when(y == 0)
    def _():
        settle()

    @pl.when(y == 1)
    def _():
        own_rest(0)
        settle()

    line_pieces(1, 0, begin, True)

    @pl.when(y == 1)
    def _():
        line_pieces(1, 1, begin, True)

    line_pieces(2, 0, begin, True)

    @pl.when(y == 0)
    def _():
        own_rest(1)
        line_pieces(1, 1, begin, True)

    cross_all(0, 0)
    cross_all(1, 0)
    cross_all(0, 1)
    for copy in w_copies:
        copy.wait()
    is_end = (chip == 0) | (chip == chips - 1)

    at_distance(0, expert)
    line_pieces(2, 1, begin, True)
    cross_all(1, 1)
    at_distance(1, expert)
    at_distance(0, lambda z: join_cores(z, False))
    for s in range(2):
        line_pieces(3, s, begin, True)
        cross_all(2, s)
    at_distance(1, join_cores)
    at_distance(2, expert)

    @pl.when(is_end)
    def _():
        send_x(chip, 1 - y)

    for s in range(2):
        cross_all(3, s)
    at_distance(2, lambda z: join_cores(z, False))

    @pl.when(jnp.logical_not(is_end))
    def _():
        for s in halves:
            at_distance(2, lambda z: send_x(z, s))
        send_x(chip, 1 - y)

    at_distance(3, expert)
    at_distance(3, join_cores)

    @pl.when(is_end)
    def _():
        for s in halves:
            at_distance(2, lambda z: send_x(z, s))

    send_x(chip, y)
    back = Line(
        chips, chip, sp, tp, lambda z: part.at[z, core, x],
        lambda z, p: part.at[z, core, x, halves[p // 2], :, columns(p, width)],
        down_in, up_in, a_sems,
    )
    def back_turn(distance, mine):
        back.send(
            jnp.where(mine, chip - distance, -1), jnp.where(mine, chip + distance, chips),
            range(PIECES), join_x,
        )

    def end(copy):
        copy.wait_send()

    def drain_dispatch():
        for h in range(2):
            end(y_copy(h))
        end(remote(sums.at[1 - core], sums_in, a_send.at[0], a_recv.at[0, 0], partner))
        mine = rows.at[:, :, core]
        end(remote(mine, mine, bulk.at[0], fan_recv.at[0], partner))
        crossed = rows.at[x, :, core]
        end(remote(crossed, crossed, bulk.at[1], fan_recv.at[0], x_peer))
        for z in range(chips):
            chunk = rows.at[x, z, core]

            @pl.when((z >= chip) & has_below)
            def _():
                end(remote(chunk, chunk, line_send.at[z, 0], fan_recv.at[0], below))

            @pl.when((z <= chip) & has_above)
            def _():
                end(remote(chunk, chunk, line_send.at[z, 1], fan_recv.at[0], above))

        end(remote(part.at[:, 1 - core], partner_in, bulk.at[2], p_recv.at[0], partner))
        drain_kv()

    mix.drain()
    back_turn(1, is_end)
    drain_dispatch()
    for distance in range(chips - 1, 1, -1):
        back_turn(distance, True)
    back_turn(1, jnp.logical_not(is_end))
    for p in range(PIECES):
        back.own(p, join_x)
        finished(p)
    def out_copy(n):
        cols = columns(n, width)
        return pltpu.make_async_copy(out_buf.at[:, cols], out_ref.at[:, cols], out_sem.at[n])

    for n in range(2):
        cols = columns(n, width)
        back_copy(n).wait_recv()
        returned = lax.dot_general(
            sel_other, y_in[:, cols], (((0,), (0,)), ((), ())), preferred_element_type=F32
        )
        out_buf[:, cols] = (total[:, cols] + returned).astype(BF16)
        out_copy(n).start()

    for n in range(2):
        end(back_copy(n))
    end(remote(part.at[:, core, 1 - x], x_in, bulk.at[3], xr_recv.at[0, 0], x_peer))
    back.drain()
    for n in range(2):
        out_copy(n).wait()


def layer_kernel(
    sp_count, chips, heads, mixer_count,
    q_hbm, k_hbm, v_hbm, res_hbm, w_hbm, gate_hbm, up_hbm, down_hbm,
    off_hbm, doc_hbm, gain_hbm, ids_hbm, group_hbm, expert_hbm,
    out_ref,
    off_ref, doc_ref, gain_ref, ids_ref, group_ref, expert_ref, table_sem,
    q_ref, k_ref, v_ref, res_ref, mixed_ref, load_sem, weight_sem, router_ref,
    gate, up, down,
    *scratch,
):
    loads = [
        pltpu.make_async_copy(src, dst, load_sem.at[n])
        for n, (src, dst) in enumerate(
            ((k_hbm, k_ref), (v_hbm, v_ref), (q_hbm, q_ref), (res_hbm, res_ref))
        )
    ]
    weights = [
        pltpu.make_async_copy(src.at[0], dst, weight_sem.at[n])
        for n, (src, dst) in enumerate(((gate_hbm, gate), (up_hbm, up), (down_hbm, down)))
    ]
    tables = [
        pltpu.make_async_copy(src, dst, table_sem.at[n])
        for n, (src, dst) in enumerate(
            (
                (off_hbm, off_ref), (doc_hbm, doc_ref), (gain_hbm, gain_ref),
                (ids_hbm, ids_ref), (group_hbm, group_ref), (expert_hbm, expert_ref),
            )
        )
    ]
    for copy in tables[:2] + loads[:3] + tables[2:]:
        copy.start()
    (
        meta_ref, doc_col, k_buf, v_buf, m_buf, acc, carry, w_buf, sums, sums_in, a_down_in, a_up_in,
        w_sem, kv_send, kv_recv, a_send, a_recv,
    ) = scratch[: mixer_count - 4]
    a_sems = scratch[mixer_count - 4 : mixer_count]
    w_copy = pltpu.make_async_copy(w_hbm, w_buf, w_sem)
    attended, drain_kv = attention(
        sp_count, chips, heads, True, tables, loads[:3], [w_copy, loads[3]] + weights,
        q_ref, k_ref, v_ref, off_ref, doc_ref,
        meta_ref, doc_col, k_buf, v_buf, m_buf, acc, carry, kv_send, kv_recv,
    )
    experts_kernel(
        chips, weights, w_copy, loads[3], attended, drain_kv,
        mixed_ref, res_ref, gain_ref, ids_ref, group_ref, expert_ref, out_ref,
        w_buf, sums, sums_in, a_down_in, a_up_in, a_send, a_recv, a_sems,
        router_ref, gate, up, down, *scratch[mixer_count:],
    )


def pair_layer(
    residual, queries, keys, values, offsets, docs, out_weight, gain,
    expert_ids, group_router, expert_router, gate, up, down,
):
    chips = lax.axis_size("tp") // 2
    rows, width = residual.shape
    heads = offsets.shape[1]
    mixer_parts = mixer_scratch(residual, queries, heads, out_weight)
    half_rows = rows // 2
    tables = (
        offsets.T, docs[None, :], gain[None, :], expert_ids.T, group_router.T, expert_router.T,
    )
    units = gate.shape[2]
    half = (chips, 2, half_rows, width)
    quarter = (chips, PIECES, half_rows, width // 2)
    dma = pltpu.SemaphoreType.DMA
    return pl.pallas_call(
        functools.partial(
            layer_kernel, lax.axis_size("sp"), chips, heads, len(mixer_parts)
        ),
        out_shape=jax.ShapeDtypeStruct((rows, width), BF16),
        in_specs=[ANY_SPEC] * 14,
        out_specs=ANY_SPEC,
        scratch_shapes=[pltpu.VMEM(table.shape, table.dtype) for table in tables]
        + [
            dma((len(tables),)),
            pltpu.VMEM(queries.shape, BF16),
            pltpu.VMEM(keys.shape, BF16),
            pltpu.VMEM(values.shape, BF16),
            pltpu.VMEM((rows, width), BF16),
            pltpu.VMEM((rows, width), BF16),
            dma((4,)),
            dma((3,)),
            pltpu.VMEM((8, width), F32),
            pltpu.VMEM((width, units), BF16),
            pltpu.VMEM((width, units), BF16),
            pltpu.VMEM((units, width), BF16),
        ]
        + mixer_parts
        + [
            pltpu.VMEM((2, chips, 2, 2, half_rows, width), BF16),
            pltpu.VMEM((half_rows, width), BF16),
            pltpu.VMEM((chips, 2, 2, 2, half_rows, width), BF16),
            pltpu.VMEM((chips, 2, 2, half_rows, width), BF16),
            pltpu.VMEM(half, BF16),
            pltpu.VMEM(quarter, BF16),
            pltpu.VMEM(quarter, BF16),
            pltpu.VMEM((half_rows, width), BF16),
            pltpu.VMEM((rows, width), F32),
            pltpu.VMEM((rows, width), BF16),
            dma((2,)),
            dma((7,)),
            dma((2, chips, 2, 2)),
            dma((chips,)),
            dma((chips, 2)),
            dma((4,)),
            dma((chips,)),
            dma((chips, 2)),
        ],
        compiler_params=pltpu.CompilerParams(
            collective_id=1, has_side_effects=True, vmem_limit_bytes=60 << 20
        ),
        name="layer",
    )(
        queries, keys, values, residual, out_weight, gate, up, down,
        *tables,
    )


def per_device(
    residual_in,
    queries,
    keys,
    values,
    break_offset,
    doc_ids,
    out_weight,
    norm_gain,
    group_router,
    expert_router,
    expert_ids,
    gate_weight,
    up_weight,
    down_weight,
):
    tok_dev = queries.shape[0]
    sp_count = lax.axis_size("sp")
    tp_count = lax.axis_size("tp")
    tp_rank = lax.axis_index("tp")
    width = residual_in.shape[1]
    rows_dev = tok_dev // tp_count
    chosen = lax.dynamic_slice_in_dim(expert_ids, tp_rank * rows_dev, rows_dev, 0)
    expert_count = sp_count * gate_weight.shape[0]
    group_size = expert_count // GROUPS
    if sp_count == 4 and gate_weight.shape[0] == 1 and rows_dev % 32 == 0:
        return pair_layer(
            residual_in, queries, keys, values, break_offset, doc_ids, out_weight, norm_gain,
            expert_ids, group_router, expert_router, gate_weight, up_weight, down_weight,
        )
    mixed_stream, normed = mixer(
        residual_in, queries, keys, values, break_offset, doc_ids, out_weight, norm_gain
    )
    routes = route_weights(normed, group_router, expert_router, chosen, group_size)
    slots = 2 * rows_dev // expert_count
    slot_ids = slot_table(chosen, expert_count, slots)
    sent = dispatch(normed, slot_ids, expert_count * slots).reshape(expert_count, slots, width)
    fanned = lax.all_gather(
        lax.all_to_all(sent, "sp", split_axis=0, concat_axis=0, tiled=True),
        "tp",
        axis=0,
        tiled=True,
    )
    partial_out = expert_rows(
        fanned.reshape(-1, width), gate_weight[0], up_weight[0], down_weight[0]
    )
    unit_total = lax.psum_scatter(
        partial_out.reshape(fanned.shape), "tp", scatter_dimension=0, tiled=True
    ).astype(jnp.float32)
    returned = lax.all_to_all(
        unit_total.astype(jnp.bfloat16), "sp", split_axis=0, concat_axis=0, tiled=True
    )
    expert_out = jnp.take(returned.reshape(-1, width), slot_ids.reshape(-1), axis=0).reshape(
        rows_dev, 2, width
    )
    mixture = jnp.sum(routes[:, :, None] * expert_out.astype(jnp.float32), axis=1)
    return (mixed_stream.astype(jnp.float32) + mixture).astype(jnp.bfloat16)


def solution(mesh):
    return jax.shard_map(
        per_device,
        mesh=mesh,
        in_specs=(
            P(("sp", "tp"), None),
            P("sp", "tp"),
            P("sp", "tp"),
            P("sp", "tp"),
            P("sp", "tp"),
            P("sp"),
            P("tp", None),
            P(),
            P(),
            P(),
            P("sp", None),
            P("sp", None, "tp"),
            P("sp", None, "tp"),
            P("sp", "tp", None),
        ),
        out_specs=P(("sp", "tp"), None),
        check_vma=False,
    )
```
